128 devices in a mesh: ep: 128 (over z, y, x, core).
Axes of the slice: x: 4, y: 4, z: 4, core: 2. Of those that a mesh axis runs over, the one named last changes fastest.
Arguments:
- tokens: bfloat16 [512, 4, 1024], P('ep'), may hold values from -6 to 6
- lengths: int32 [512], P('ep'), may hold values from 1 to 4, 768 in all
- routes: int32 [512, 4, 8], P('ep'), may hold values from 0 to 255, all different within a row; in each aligned block of 16 rows (0 to 15, 16 to 31, ...) at most 4 rows name the same one
- gates: float32 [512, 4, 8], P('ep'), may hold values from 0.05 to 0.6
- norm_gain: float32 [1024], replicated, may hold values from 0.5 to 1.5
- expert_gate: bfloat16 [256, 1024, 256], P('ep'), may hold values from -0.1875 to 0.1875
- expert_up: bfloat16 [256, 1024, 256], P('ep'), may hold values from -0.1875 to 0.1875
- expert_down: bfloat16 [256, 256, 1024], P('ep'), may hold values from -0.375 to 0.375
- shared_gate: bfloat16 [1024, 256], replicated, may hold values from -0.1875 to 0.1875
- shared_up: bfloat16 [1024, 256], replicated, may hold values from -0.1875 to 0.1875
- shared_down: bfloat16 [256, 1024], replicated, may hold values from -0.375 to 0.375
- out_gain: float32 [1024], replicated, may hold values from 0.5 to 1.5
Outputs:
- mixed: bfloat16 [512, 4, 1024], P('ep')
The draws below stay inside these ranges and needn't reach their ends.
Inputs may be any that keep to these rules, and one draw needn't show every extreme that they name: `routes`: in the 16 rows of one device (all slots, in order), no expert is named by more than 4 rows, and some device reaches 4; the experts of one row differ. `lengths`: each sequence has 1 to 4 live slots, the longest exactly 4.
All inputs are finite; a program needn't handle non-finite values.
Results may differ from the reference program's by a relative error of at most 0.0065.
Values may be sent and summed in bfloat16 or wider, within the bound.
A program may use at most 64 MiB of HBM per device.

```python
import math
import jax
import jax.numpy as jnp
import numpy as np
from jax import lax

D = 1024
FF = 256
SFF = 256
TOP = 8
NEW = 4
MOST = 4
SEQUENCES = 512
TOK_DEV = 16
EXPERTS = 256


def block_scale(rng, shape, split, smallest, high):
    factor_of, own = 1.0, jax.random.fold_in(rng, 6)
    for position, parts in split:
        heights = jnp.exp(jax.random.uniform(jax.random.fold_in(own, position), (parts,), jnp.float32, smallest / len(split), high / len(split)))
        factor_of = factor_of * jnp.repeat(heights, shape[position] // parts).reshape([-1 if axis == position else 1 for axis in range(len(shape))])
    return factor_of


def length_profile(number_of, total, most, skew):
    portions = [(1 << 20) // math.isqrt(rank ** skew) + 1 for rank in range(2, number_of + 1)]
    surplus, given = total - most - (number_of - 1), [1] * (number_of - 1)
    while surplus > 0:
        free = [i for i in range(number_of - 1) if given[i] < most]
        whole, remaining = sum([portions[i] for i in free]), surplus
        for i in free:
            addition = min(most - given[i], max(1, remaining * portions[i] // whole), surplus)
            given[i] = given[i] + addition
            surplus = surplus - addition
    return np.array([most] + given)


def uneven(rng, amount, total, most, lean):
    if amount == 2:
        one = jax.random.randint(rng, (), max(1, total - most), min(most, total - 1) + 1)
        return jnp.stack([one, total - one])
    sizes = jnp.asarray(length_profile(amount, total, most, lean), jnp.int32)
    twos = (amount - 1) // 2
    donor, sink = sizes[1:1 + 2 * twos:2], sizes[2:2 + 2 * twos:2]
    slack = jnp.minimum(donor - 1, most - sink)
    passed = jax.random.randint(jax.random.fold_in(rng, 1), (twos,), 0, 1 << 20) % (slack + 1)
    sizes = sizes.at[1:1 + 2 * twos:2].set(donor - passed).at[2:2 + 2 * twos:2].set(sink + passed)
    return sizes[jax.random.permutation(jax.random.fold_in(rng, 2), amount)]


def shared_out(key, own, number, rows, number_of, top, limit, slope):
    sequence = jax.random.permutation(key, number_of)
    heavy_load, usual = portions_of(number_of, rows * top, limit, slope, True), portions_of(number_of, rows * top, limit, slope, False)
    places = jnp.arange(number_of)

    def named(sizes, rotation):
        used = int((sizes > 0).sum())
        fixed = max(1, used // 4)
        passed = fixed + (places - fixed + rotation * (used - fixed)) % max(1, number_of - fixed)
        return jnp.zeros((number_of,), jnp.int32).at[sequence[jnp.where(places < fixed, places, passed)]].set(jnp.asarray(sizes, jnp.int32))

    sizes = jnp.where(number % 4 == 0, named(heavy_load, number // 4), named(usual, number - number // 4 - 1))
    mixed = jax.random.permutation(jax.random.fold_in(own, 3), number_of)
    donor, sink = mixed[0:number_of // 2 * 2:2], mixed[1:number_of // 2 * 2:2]
    room = jnp.minimum(sizes[donor] - 1, limit - sizes[sink]) // 2
    room = jnp.where((donor == sequence[0]) | (sink == sequence[0]) | (sizes[sink] == 0), 0, jnp.maximum(room, 0))
    passed = jax.random.randint(jax.random.fold_in(own, 4), (number_of // 2,), 0, 1 << 20) % (room + 1)
    sizes = sizes.at[donor].add(-passed).at[sink].add(passed)
    members = jnp.searchsorted(jnp.cumsum(sizes), jnp.arange(rows * top), side="right").astype(jnp.int32)
    grid = members.reshape(top, rows).T
    grid = grid[jax.random.permutation(jax.random.fold_in(own, 1), rows)]
    rotation = jax.random.randint(jax.random.fold_in(own, 2), (rows, 1), 0, top)
    return jnp.take_along_axis(grid, (jnp.arange(top)[None, :] + rotation) % top, axis=1)


def portions_of(number_of, total, limit, lean, full):
    portions = [(1 << 20) // math.isqrt(standing ** lean) + 1 for standing in range(1, number_of + 1)]
    largest = limit if full else min(limit, max(-(-total // number_of), total * portions[0] // sum(portions)))
    least = 1 if total - largest >= number_of - 1 else 0
    holding, rest = [largest] + [least] * (number_of - 1), total - largest - least * (number_of - 1)
    while rest > 0:
        free = [i for i in range(1, number_of) if holding[i] < largest] or [i for i in range(1, number_of) if holding[i] < limit]
        whole, budget = sum([portions[i] for i in free]), rest
        for i in free:
            addition = min(limit - holding[i], max(1, budget * portions[i] // whole), rest)
            holding[i] = holding[i] + addition
            rest = rest - addition
    return np.array(holding)


def centred(own_key, shape, spread, bound, shards=(), kind=jnp.bfloat16):
    entries = jax.random.normal(own_key, shape, jnp.float32) * spread
    if len(shards) > 0:
        entries = block_scale(own_key, shape, shards, -0.22, 0.18) * entries
    return jnp.clip(entries, min=-bound, max=bound).astype(kind)


def setup_inputs(seed: int = 0) -> dict:
    streams_of = jax.random.split(jax.random.key(seed), 13)
    tokens = centred(streams_of[0], (SEQUENCES, NEW, D), 1.0, 6.0, ((0, 128),))
    lengths = uneven(streams_of[1], SEQUENCES, SEQUENCES * 3 // 2, NEW, 2).astype(jnp.int32)
    routes_keys = jax.random.split(jax.random.fold_in(streams_of[2], 1), SEQUENCES * NEW // TOK_DEV)
    routes_turns = jax.random.permutation(jax.random.fold_in(streams_of[2], 3), SEQUENCES * NEW // TOK_DEV)
    routes = jax.vmap(lambda own, number: shared_out(jax.random.fold_in(streams_of[2], 2), own, number, TOK_DEV, EXPERTS, TOP, MOST, 2))(routes_keys, routes_turns).reshape((SEQUENCES, NEW, TOP))
    gates = jnp.clip(0.05 + 0.55 * jax.random.uniform(streams_of[3], (SEQUENCES, NEW, TOP), jnp.float32) ** block_scale(streams_of[3], (SEQUENCES, NEW, TOP), ((0, 128),), -0.2, 0.2), 0.05, 0.6)
    norm_gain = jnp.clip(1.0 + 0.1 * jax.random.normal(streams_of[4], (D,), jnp.float32), 0.5, 1.5)
    expert_gate = centred(streams_of[5], (EXPERTS, D, FF), D ** -0.5, 0.1875, ((0, 128),))
    expert_up = centred(streams_of[6], (EXPERTS, D, FF), D ** -0.5, 0.1875, ((0, 128),))
    expert_down = centred(streams_of[7], (EXPERTS, FF, D), FF ** -0.5, 0.375, ((0, 128),))
    shared_gate = centred(streams_of[8], (D, SFF), D ** -0.5, 0.1875)
    shared_up = centred(streams_of[9], (D, SFF), D ** -0.5, 0.1875)
    shared_down = centred(streams_of[10], (SFF, D), SFF ** -0.5, 0.375)
    out_gain = jnp.clip(1.0 + 0.1 * jax.random.normal(streams_of[11], (D,), jnp.float32), 0.5, 1.5)
    return {"tokens": tokens, "lengths": lengths, "routes": routes, "gates": gates, "norm_gain": norm_gain, "expert_gate": expert_gate, "expert_up": expert_up, "expert_down": expert_down, "shared_gate": shared_gate, "shared_up": shared_up, "shared_down": shared_down, "out_gain": out_gain}


EPS = 1e-06

def norm_rows(values, scales):
    wide = values.astype(jnp.float32)
    return wide * lax.rsqrt(lax.optimization_barrier(jnp.mean(wide * wide, axis=-1, keepdims=True)) + EPS) * scales

def reference(tokens, lengths, routes, gates, norm_gain, expert_gate, expert_up, expert_down, shared_gate, shared_up, shared_down, out_gain):
    features = tokens.shape[-1]
    flat_rows = tokens.reshape(-1, features)
    normed = norm_rows(flat_rows, norm_gain).astype(jnp.bfloat16)
    live_mask = (jnp.arange(NEW, dtype=jnp.int32)[None, :] < lengths[:, None]).reshape(-1)
    expert_ids = routes.reshape(-1)
    copies = jnp.repeat(normed, TOP, axis=0)
    block_rows = 32
    row_blocks = copies.reshape(-1, block_rows, features)
    id_blocks = expert_ids.reshape(-1, block_rows)

    def one_block(pair):
        rows_in, ids_in = pair
        wide_rows = rows_in.astype(jnp.float32)
        gate_part = jnp.einsum('rd,rdf->rf', wide_rows, expert_gate[ids_in].astype(jnp.float32))
        up_part = jnp.einsum('rd,rdf->rf', wide_rows, expert_up[ids_in].astype(jnp.float32))
        hidden = (jax.nn.silu(gate_part) * up_part).astype(jnp.bfloat16)
        result = jnp.einsum('rf,rfd->rd', hidden.astype(jnp.float32), expert_down[ids_in].astype(jnp.float32))
        return result.astype(jnp.bfloat16)
    outputs = lax.map(one_block, (row_blocks, id_blocks)).reshape(-1, TOP, features)
    weights = jnp.where(live_mask[:, None], gates.reshape(-1, TOP), jnp.float32(0.0))
    routed = lax.optimization_barrier(jnp.sum(weights[:, :, None] * outputs.astype(jnp.float32), axis=1))
    shared_hidden = (jax.nn.silu(jnp.dot(normed, shared_gate, preferred_element_type=jnp.float32)) * jnp.dot(normed, shared_up, preferred_element_type=jnp.float32)).astype(jnp.bfloat16)
    shared = jnp.dot(shared_hidden, shared_down, preferred_element_type=jnp.float32)
    summed = routed + shared
    mixed_out = jnp.where(live_mask[:, None], norm_rows(summed, out_gain), jnp.float32(0.0))
    return mixed_out.astype(jnp.bfloat16).reshape(tokens.shape)
```

```python
import jax
import jax.numpy as jnp
from jax import lax
from jax.experimental import pallas as pl
from jax.experimental.pallas import tpu as pltpu
from jax.sharding import PartitionSpec as P

MESH = pl.DeviceIdType.MESH
EPS = 1e-06
BF = jnp.bfloat16
F32 = jnp.float32
D = 1024
WIDE = 1152
CUT = 384
WIDTH = (384, 384, 256)
ORDER = (0, 1, 3, 2)


def kernel(
    lengths_ref, tokens_ref, routes_ref, gates_ref, ng_ref, og_ref,
    eg_ref, eu_ref, ed_ref, sg_ref, su_ref, sd_ref,
    out_ref,
    xg, yb, r1a, r1b, r1c, s1a, s1b, s1c, r2a, r2b, r2c, s2a, s2b, s2c, r3a, r3b, r3c,
    wg, wu, wd, sgv, suv, sdv, rows, meta_a, meta_b, hs, total,
    ag_send, ag_recv, rs_send, rs_recv, w_send, w_recv, w_local,
):
    me = lax.axis_index("ep")
    core = lax.rem(me, 2)
    chip = me // 2
    c = (chip // 16, lax.rem(chip // 4, 4), lax.rem(chip, 4))
    stride = (32, 8, 2)
    partner = me + 1 - 2 * core

    def shifted(dim, o):
        return lax.rem(c[dim] + o, 4)

    def device(dim, o):
        return me + (shifted(dim, o) - c[dim]) * stride[dim]

    barrier = pltpu.get_barrier_semaphore()
    pl.semaphore_signal(barrier, inc=1, device_id=(partner,), device_id_type=MESH)
    for dim in range(3):
        for o in (1, 2, 3):
            pl.semaphore_signal(
                barrier, inc=1, device_id=(device(dim, o),), device_id_type=MESH
            )

    mine = pl.ds(2 * core, 2)
    local = []
    for n, (src, dst) in enumerate(
        (
            (eg_ref, wg.at[mine]), (eu_ref, wu.at[mine]), (ed_ref, wd.at[mine]),
            (sg_ref, sgv), (su_ref, suv), (sd_ref, sdv),
        )
    ):
        copy = pltpu.make_async_copy(src, dst, w_local.at[n])
        copy.start()
        local.append(copy)

    row = lax.broadcasted_iota(jnp.int32, (16, 1), 0)
    limit = jnp.zeros((16, 1), jnp.int32)
    for s in range(4):
        limit = jnp.where(row // 4 == s, lengths_ref[s], limit)
        rows[4 * s : 4 * s + 4, :] = tokens_ref[s].astype(F32)
        meta_a[4 * s : 4 * s + 4, 0:8] = routes_ref[s].astype(F32)
        meta_b[4 * s : 4 * s + 4, 0:8] = gates_ref[s]
    live = lax.rem(row, 4) < limit
    values = rows[...]
    mean = jnp.mean(values * values, axis=-1, keepdims=True)
    normed = (values * lax.rsqrt(mean + EPS) * ng_ref[...]).astype(BF)
    lane = lax.broadcasted_iota(jnp.int32, (16, 128), 1)
    ids = jnp.where(live, meta_a[...], -1.0)
    gate = meta_b[...]
    high = gate.astype(BF).astype(F32)
    low = gate - high
    packed = jnp.where(
        lane < 8,
        ids,
        jnp.where(
            lane < 16,
            pltpu.roll(high, 8, 1),
            jnp.where(lane < 24, pltpu.roll(low, 16, 1), 0.0),
        ),
    )
    xg[c[0], c[1], c[2], :, 0:D] = normed
    xg[c[0], c[1], c[2], :, D:WIDE] = packed.astype(BF)

    pl.semaphore_wait(barrier, 10)

    def swap(n, dst_slot):
        src, dst = ((eg_ref, wg), (eu_ref, wu), (ed_ref, wd))[n]
        return pltpu.make_async_remote_copy(
            src_ref=src, dst_ref=dst.at[dst_slot], send_sem=w_send.at[n],
            recv_sem=w_recv.at[n], device_id=(partner,), device_id_type=MESH,
        )

    theirs = pl.ds(2 - 2 * core, 2)

    def ag(stage, part, o, sub=None, incoming=False):
        dim = (part + stage) % 3
        index = [c[0], c[1], c[2]]
        for t in range(stage):
            index[(part + t) % 3] = slice(None)
        if sub is not None:
            index[0] = lax.rem(c[0] + sub, 4)
        if incoming:
            index[dim] = shifted(dim, 4 - o)
        ref = xg.at[index[0], index[1], index[2], :, pl.ds(CUT * part, CUT)]
        if stage < 2:
            n = stage * 9 + part * 3 + o - 1
        elif part == 1:
            n = 42 + o - 1
        else:
            n = 18 + (12 if part == 2 else 0) + sub * 3 + o - 1
        return pltpu.make_async_remote_copy(
            src_ref=ref, dst_ref=ref, send_sem=ag_send.at[n], recv_sem=ag_recv.at[n],
            device_id=(device(dim, o),), device_id_type=MESH,
        )

    sent = []

    def go(copy):
        copy.start()
        sent.append(copy)

    for part in range(3):
        for o in (1, 3, 2):
            go(ag(0, part, o))
    for n in range(3):
        go(swap(n, mine))
    for part in range(3):
        for o in (1, 3, 2):
            ag(0, part, o, incoming=True).wait_recv()
        for o in (1, 3, 2):
            go(ag(1, part, o))
    for part in (1, 0, 2):
        for o in (1, 3, 2):
            ag(1, part, o, incoming=True).wait_recv()
        if part == 1:
            for o in (1, 3, 2):
                go(ag(2, 1, o))
        else:
            for sub in ORDER:
                for o in (1, 3, 2):
                    go(ag(2, part, o, sub=sub))

    for copy in local:
        copy.wait()
    own = xg[c[0], c[1], c[2], :, 0:D]
    part_g = jnp.dot(own, sgv[...], preferred_element_type=F32)
    part_u = jnp.dot(own, suv[...], preferred_element_type=F32)
    hidden = (part_g / (1.0 + jnp.exp(-part_g)) * part_u).astype(BF)
    total[...] = jnp.dot(hidden, sdv[...], preferred_element_type=F32)

    for n in range(3):
        swap(n, theirs).wait_recv()

    r1, s1 = (r1a, r1b, r1c), (s1a, s1b, s1c)
    r2, s2 = (r2a, r2b, r2c), (s2a, s2b, s2c)
    r3 = (r3a, r3b, r3c)

    def columns(part):
        return pl.ds(CUT * part, WIDTH[part])

    def rs1(part, o, sub=None):
        dim = (part + 2) % 3
        to = shifted(dim, o)
        k = None if sub is None else lax.rem(c[0] + sub, 4)
        if part == 0:
            src, dst = yb.at[k, :, to, :, columns(0)], r1a.at[o - 1, k]
            n = sub * 3 + o - 1
        elif part == 1:
            src, dst = yb.at[to, :, :, :, columns(1)], r1b.at[o - 1]
            n = 24 + o - 1
        else:
            src, dst = yb.at[k, to, :, :, columns(2)], r1c.at[o - 1, k]
            n = 12 + sub * 3 + o - 1
        return pltpu.make_async_remote_copy(
            src_ref=src, dst_ref=dst, send_sem=rs_send.at[n], recv_sem=rs_recv.at[n],
            device_id=(device(dim, o),), device_id_type=MESH,
        )

    def rs2(part, o):
        dim = (part + 1) % 3
        to = shifted(dim, o)
        src = s1[part].at[to] if part == 2 else s1[part].at[:, to]
        n = 27 + part * 3 + o - 1
        return pltpu.make_async_remote_copy(
            src_ref=src, dst_ref=r2[part].at[o - 1], send_sem=rs_send.at[n],
            recv_sem=rs_recv.at[n], device_id=(device(dim, o),), device_id_type=MESH,
        )

    def rs3(part, o):
        dim = part
        n = 36 + part * 3 + o - 1
        return pltpu.make_async_remote_copy(
            src_ref=s2[part].at[shifted(dim, o)], dst_ref=r3[part].at[o - 1],
            send_sem=rs_send.at[n], recv_sem=rs_recv.at[n],
            device_id=(device(dim, o),), device_id_type=MESH,
        )

    wide_lane = lax.broadcasted_iota(jnp.int32, (256, 128), 1)
    for off in ORDER:
        k = lax.rem(c[0] + off, 4)
        for o in (1, 3, 2):
            ag(2, 0, o, sub=off, incoming=True).wait_recv()
            ag(2, 2, o, sub=off, incoming=True).wait_recv()
        if off != 0:
            ag(2, 1, 4 - off, incoming=True).wait_recv()
        info = xg[k, :, :, :, D:WIDE].reshape(256, 128).astype(F32)
        weights = pltpu.roll(info, 120, 1) + pltpu.roll(info, 112, 1)
        x = xg[k, :, :, :, 0:D].reshape(256, D)
        for e in range(4):
            name = (4 * chip + e).astype(F32)
            hit = jnp.where((info == name) & (wide_lane < 8), weights, 0.0)
            w = jnp.sum(hit, axis=1, keepdims=True)
            g = jnp.dot(x, wg[e], preferred_element_type=F32)
            u = jnp.dot(x, wu[e], preferred_element_type=F32)
            hs[:, 256 * e : 256 * e + 256] = (g / (1.0 + jnp.exp(-g)) * u * w).astype(BF)
        y = jnp.dot(hs[...], wd[...].reshape(D, D), preferred_element_type=F32)
        yb[k] = y.astype(BF).reshape(4, 4, 16, D)
        for o in (1, 3, 2):
            go(rs1(0, o, sub=off))
            go(rs1(2, o, sub=off))
        if off != 0:
            go(rs1(1, off))

    for part in (0, 2, 1):
        for o in (1, 3, 2):
            if part == 1:
                rs1(1, o).wait_recv()
            else:
                for sub in ORDER:
                    rs1(part, o, sub=sub).wait_recv()
        if part == 0:
            base = yb[:, :, c[2], :, columns(0)]
        elif part == 1:
            base = yb[c[0], :, :, :, columns(1)]
        else:
            base = yb[:, c[1], :, :, columns(2)]
        acc = base.astype(F32)
        for o in (1, 2, 3):
            acc = acc + r1[part][o - 1].astype(F32)
        s1[part][...] = acc.astype(BF)
        for o in (1, 3, 2):
            go(rs2(part, o))
    for part in (0, 2, 1):
        for o in (1, 3, 2):
            rs2(part, o).wait_recv()
        dim = (part + 1) % 3
        base = s1[part][c[dim]] if part == 2 else s1[part][:, c[dim]]
        acc = base.astype(F32)
        for o in (1, 2, 3):
            acc = acc + r2[part][o - 1].astype(F32)
        s2[part][...] = acc.astype(BF)
        for o in (1, 3, 2):
            go(rs3(part, o))
    for part in (0, 2, 1):
        for o in (1, 3, 2):
            rs3(part, o).wait_recv()
        acc = s2[part][c[part]].astype(F32)
        for o in (1, 2, 3):
            acc = acc + r3[part][o - 1].astype(F32)
        total[:, CUT * part : CUT * part + WIDTH[part]] += acc

    summed = total[...]
    mean = jnp.mean(summed * summed, axis=-1, keepdims=True)
    mixed = jnp.where(live, summed * lax.rsqrt(mean + EPS) * og_ref[...], 0.0)
    mixed = mixed.astype(BF)
    for s in range(4):
        out_ref[s] = mixed[4 * s : 4 * s + 4, :]
    for copy in sent:
        copy.wait_send()


def per_device(
    tokens, lengths, routes, gates, norm_gain,
    expert_gate, expert_up, expert_down, shared_gate, shared_up, shared_down, out_gain,
):
    vmem = pl.BlockSpec(memory_space=pltpu.VMEM)
    hbm = pl.BlockSpec(memory_space=pl.ANY)
    dma = pltpu.SemaphoreType.DMA
    buffers = [pltpu.VMEM((4, 4, 4, 16, WIDE), BF), pltpu.VMEM((4, 4, 4, 16, D), BF)]
    buffers += [pltpu.VMEM((3, 4, 4, 16, w), BF) for w in WIDTH]
    buffers += [pltpu.VMEM((4, 4, 16, w), BF) for w in WIDTH]
    buffers += [pltpu.VMEM((3, 4, 16, w), BF) for w in WIDTH]
    buffers += [pltpu.VMEM((4, 16, w), BF) for w in WIDTH]
    buffers += [pltpu.VMEM((3, 16, w), BF) for w in WIDTH]
    buffers += [
        pltpu.VMEM((4, D, 256), BF), pltpu.VMEM((4, D, 256), BF), pltpu.VMEM((4, 256, D), BF),
        pltpu.VMEM((D, 256), BF), pltpu.VMEM((D, 256), BF), pltpu.VMEM((256, D), BF),
        pltpu.VMEM((16, D), F32), pltpu.VMEM((16, 128), F32), pltpu.VMEM((16, 128), F32),
        pltpu.VMEM((256, D), BF), pltpu.VMEM((16, D), F32),
    ]
    return pl.pallas_call(
        kernel,
        out_shape=jax.ShapeDtypeStruct(tokens.shape, BF),
        in_specs=[pl.BlockSpec(memory_space=pltpu.SMEM)] + [vmem] * 5 + [hbm] * 6,
        out_specs=vmem,
        scratch_shapes=buffers
        + [dma((45,)), dma((45,)), dma((45,)), dma((45,)), dma((3,)), dma((3,)), dma((6,))],
        compiler_params=pltpu.CompilerParams(
            collective_id=0, has_side_effects=True, vmem_limit_bytes=48 * 2**20
        ),
    )(
        lengths, tokens, routes, gates, norm_gain.reshape(1, D), out_gain.reshape(1, D),
        expert_gate, expert_up, expert_down, shared_gate, shared_up, shared_down,
    )


def solution(mesh):
    placed = (
        P("ep", None, None), P("ep"), P("ep", None, None), P("ep", None, None), P(),
        P("ep", None, None), P("ep", None, None), P("ep", None, None), P(), P(), P(), P(),
    )
    return jax.shard_map(
        per_device, mesh=mesh, in_specs=placed, out_specs=P("ep", None, None), check_vma=False
    )
```

```python
import jax
import jax.numpy as jnp
from jax import lax
from jax.experimental import pallas as pl
from jax.experimental.pallas import tpu as pltpu
from jax.sharding import PartitionSpec as P

MESH = pl.DeviceIdType.MESH
EPS = 1e-06
BF = jnp.bfloat16
F32 = jnp.float32
D = 1024
WIDE = 1152
CUT = 384
WIDTH = (384, 384, 256)
ORDER = (0, 1, 3, 2)


def kernel(
    lengths_hbm, tokens_hbm, routes_hbm, gates_hbm, ng_hbm, og_hbm,
    eg_ref, eu_ref, ed_ref, sg_ref, su_ref, sd_ref,
    out_ref,
    xg, yb, r1a, r1b, r1c, s1a, s1b, s1c, r2a, r2b, r2c, s2a, s2b, s2c, r3a, r3b, r3c,
    wg, wu, wd, sgv, suv, sdv, rows, meta_a, meta_b, hs, total,
    lengths_ref, tokens_ref, routes_ref, gates_ref, ng_ref, og_ref,
    ag_send, ag_recv, rs_send, rs_recv, w_send, w_recv, w_local, small,
):
    me = lax.axis_index("ep")
    core = lax.rem(me, 2)
    chip = me // 2
    c = (chip // 16, lax.rem(chip // 4, 4), lax.rem(chip, 4))
    stride = (32, 8, 2)
    partner = me + 1 - 2 * core

    def shifted(dim, o):
        return lax.rem(c[dim] + o, 4)

    def device(dim, o):
        return me + (shifted(dim, o) - c[dim]) * stride[dim]

    barrier = pltpu.get_barrier_semaphore()
    pl.semaphore_signal(barrier, inc=1, device_id=(partner,), device_id_type=MESH)
    for dim in range(3):
        for o in (1, 2, 3):
            pl.semaphore_signal(
                barrier, inc=1, device_id=(device(dim, o),), device_id_type=MESH
            )

    early = []
    for n, (src, dst) in enumerate(
        (
            (tokens_hbm, tokens_ref), (ng_hbm, ng_ref), (routes_hbm, routes_ref),
            (gates_hbm, gates_ref), (lengths_hbm, lengths_ref), (og_hbm, og_ref),
        )
    ):
        copy = pltpu.make_async_copy(src, dst, small.at[n])
        copy.start()
        early.append(copy)
    mine = pl.ds(2 * core, 2)
    local = []
    for n, (src, dst) in enumerate(
        (
            (eg_ref, wg.at[mine]), (eu_ref, wu.at[mine]), (ed_ref, wd.at[mine]),
            (sg_ref, sgv), (su_ref, suv), (sd_ref, sdv),
        )
    ):
        copy = pltpu.make_async_copy(src, dst, w_local.at[n])
        copy.start()
        local.append(copy)

    for copy in early:
        copy.wait()
    row = lax.broadcasted_iota(jnp.int32, (16, 1), 0)
    limit = jnp.zeros((16, 1), jnp.int32)
    for s in range(4):
        limit = jnp.where(row // 4 == s, lengths_ref[s], limit)
        rows[4 * s : 4 * s + 4, :] = tokens_ref[s].astype(F32)
        meta_a[4 * s : 4 * s + 4, 0:8] = routes_ref[s].astype(F32)
        meta_b[4 * s : 4 * s + 4, 0:8] = gates_ref[s]
    live = lax.rem(row, 4) < limit
    values = rows[...]
    mean = jnp.mean(values * values, axis=-1, keepdims=True)
    normed = (values * lax.rsqrt(mean + EPS) * ng_ref[...]).astype(BF)
    lane = lax.broadcasted_iota(jnp.int32, (16, 128), 1)
    ids = jnp.where(live, meta_a[...], -1.0)
    gate = meta_b[...]
    high = gate.astype(BF).astype(F32)
    low = gate - high
    packed = jnp.where(
        lane < 8,
        ids,
        jnp.where(
            lane < 16,
            pltpu.roll(high, 8, 1),
            jnp.where(lane < 24, pltpu.roll(low, 16, 1), 0.0),
        ),
    )
    xg[c[0], c[1], c[2], :, 0:D] = normed
    xg[c[0], c[1], c[2], :, D:WIDE] = packed.astype(BF)

    pl.semaphore_wait(barrier, 10)

    def swap(n, dst_slot):
        src, dst = ((eg_ref, wg), (eu_ref, wu), (ed_ref, wd))[n]
        return pltpu.make_async_remote_copy(
            src_ref=src, dst_ref=dst.at[dst_slot], send_sem=w_send.at[n],
            recv_sem=w_recv.at[n], device_id=(partner,), device_id_type=MESH,
        )

    theirs = pl.ds(2 - 2 * core, 2)

    def ag(stage, part, o, sub=None, incoming=False):
        dim = (part + stage) % 3
        index = [c[0], c[1], c[2]]
        for t in range(stage):
            index[(part + t) % 3] = slice(None)
        if sub is not None:
            index[0] = lax.rem(c[0] + sub, 4)
        if incoming:
            index[dim] = shifted(dim, 4 - o)
        ref = xg.at[index[0], index[1], index[2], :, pl.ds(CUT * part, CUT)]
        if stage < 2:
            n = stage * 9 + part * 3 + o - 1
        elif part == 1:
            n = 42 + o - 1
        else:
            n = 18 + (12 if part == 2 else 0) + sub * 3 + o - 1
        return pltpu.make_async_remote_copy(
            src_ref=ref, dst_ref=ref, send_sem=ag_send.at[n], recv_sem=ag_recv.at[n],
            device_id=(device(dim, o),), device_id_type=MESH,
        )

    sent = []

    def go(copy):
        copy.start()
        sent.append(copy)

    for part in range(3):
        for o in (1, 3, 2):
            go(ag(0, part, o))
    for n in range(3):
        go(swap(n, mine))
    for part in range(3):
        for o in (1, 3, 2):
            ag(0, part, o, incoming=True).wait_recv()
        for o in (1, 3, 2):
            go(ag(1, part, o))
    for part in (1, 0, 2):
        for o in (1, 3, 2):
            ag(1, part, o, incoming=True).wait_recv()
        if part == 1:
            for o in (1, 3, 2):
                go(ag(2, 1, o))
        else:
            for sub in ORDER:
                for o in (1, 3, 2):
                    go(ag(2, part, o, sub=sub))

    for copy in local:
        copy.wait()
    own = xg[c[0], c[1], c[2], :, 0:D]
    part_g = jnp.dot(own, sgv[...], preferred_element_type=F32)
    part_u = jnp.dot(own, suv[...], preferred_element_type=F32)
    hidden = (part_g / (1.0 + jnp.exp(-part_g)) * part_u).astype(BF)
    total[...] = jnp.dot(hidden, sdv[...], preferred_element_type=F32)

    for n in range(3):
        swap(n, theirs).wait_recv()

    r1, s1 = (r1a, r1b, r1c), (s1a, s1b, s1c)
    r2, s2 = (r2a, r2b, r2c), (s2a, s2b, s2c)
    r3 = (r3a, r3b, r3c)

    def columns(part):
        return pl.ds(CUT * part, WIDTH[part])

    def rs1(part, o, sub=None):
        dim = (part + 2) % 3
        to = shifted(dim, o)
        k = None if sub is None else lax.rem(c[0] + sub, 4)
        if part == 0:
            src, dst = yb.at[k, :, to, :, columns(0)], r1a.at[o - 1, k]
            n = sub * 3 + o - 1
        elif part == 1:
            src, dst = yb.at[to, :, :, :, columns(1)], r1b.at[o - 1]
            n = 24 + o - 1
        else:
            src, dst = yb.at[k, to, :, :, columns(2)], r1c.at[o - 1, k]
            n = 12 + sub * 3 + o - 1
        return pltpu.make_async_remote_copy(
            src_ref=src, dst_ref=dst, send_sem=rs_send.at[n], recv_sem=rs_recv.at[n],
            device_id=(device(dim, o),), device_id_type=MESH,
        )

    def rs2(part, o):
        dim = (part + 1) % 3
        to = shifted(dim, o)
        src = s1[part].at[to] if part == 2 else s1[part].at[:, to]
        n = 27 + part * 3 + o - 1
        return pltpu.make_async_remote_copy(
            src_ref=src, dst_ref=r2[part].at[o - 1], send_sem=rs_send.at[n],
            recv_sem=rs_recv.at[n], device_id=(device(dim, o),), device_id_type=MESH,
        )

    def rs3(part, o):
        dim = part
        n = 36 + part * 3 + o - 1
        return pltpu.make_async_remote_copy(
            src_ref=s2[part].at[shifted(dim, o)], dst_ref=r3[part].at[o - 1],
            send_sem=rs_send.at[n], recv_sem=rs_recv.at[n],
            device_id=(device(dim, o),), device_id_type=MESH,
        )

    wide_lane = lax.broadcasted_iota(jnp.int32, (256, 128), 1)
    for off in ORDER:
        k = lax.rem(c[0] + off, 4)
        for o in (1, 3, 2):
            ag(2, 0, o, sub=off, incoming=True).wait_recv()
            ag(2, 2, o, sub=off, incoming=True).wait_recv()
        if off != 0:
            ag(2, 1, 4 - off, incoming=True).wait_recv()
        info = xg[k, :, :, :, D:WIDE].reshape(256, 128).astype(F32)
        weights = pltpu.roll(info, 120, 1) + pltpu.roll(info, 112, 1)
        x = xg[k, :, :, :, 0:D].reshape(256, D)
        for e in range(4):
            name = (4 * chip + e).astype(F32)
            hit = jnp.where((info == name) & (wide_lane < 8), weights, 0.0)
            w = jnp.sum(hit, axis=1, keepdims=True)
            g = jnp.dot(x, wg[e], preferred_element_type=F32)
            u = jnp.dot(x, wu[e], preferred_element_type=F32)
            hs[:, 256 * e : 256 * e + 256] = (g / (1.0 + jnp.exp(-g)) * u * w).astype(BF)
        y = jnp.dot(hs[...], wd[...].reshape(D, D), preferred_element_type=F32)
        yb[k] = y.astype(BF).reshape(4, 4, 16, D)
        for o in (1, 3, 2):
            go(rs1(0, o, sub=off))
            go(rs1(2, o, sub=off))
        if off != 0:
            go(rs1(1, off))

    for part in (0, 2, 1):
        for o in (1, 3, 2):
            if part == 1:
                rs1(1, o).wait_recv()
            else:
                for sub in ORDER:
                    rs1(part, o, sub=sub).wait_recv()
        if part == 0:
            base = yb[:, :, c[2], :, columns(0)]
        elif part == 1:
            base = yb[c[0], :, :, :, columns(1)]
        else:
            base = yb[:, c[1], :, :, columns(2)]
        acc = base.astype(F32)
        for o in (1, 2, 3):
            acc = acc + r1[part][o - 1].astype(F32)
        s1[part][...] = acc.astype(BF)
        for o in (1, 3, 2):
            go(rs2(part, o))
    for part in (0, 2, 1):
        for o in (1, 3, 2):
            rs2(part, o).wait_recv()
        dim = (part + 1) % 3
        base = s1[part][c[dim]] if part == 2 else s1[part][:, c[dim]]
        acc = base.astype(F32)
        for o in (1, 2, 3):
            acc = acc + r2[part][o - 1].astype(F32)
        s2[part][...] = acc.astype(BF)
        for o in (1, 3, 2):
            go(rs3(part, o))
    for part in (0, 2, 1):
        for o in (1, 3, 2):
            rs3(part, o).wait_recv()
        acc = s2[part][c[part]].astype(F32)
        for o in (1, 2, 3):
            acc = acc + r3[part][o - 1].astype(F32)
        total[:, CUT * part : CUT * part + WIDTH[part]] += acc

    summed = total[...]
    mean = jnp.mean(summed * summed, axis=-1, keepdims=True)
    mixed = jnp.where(live, summed * lax.rsqrt(mean + EPS) * og_ref[...], 0.0)
    mixed = mixed.astype(BF)
    for s in range(4):
        out_ref[s] = mixed[4 * s : 4 * s + 4, :]
    for copy in sent:
        copy.wait_send()


def per_device(
    tokens, lengths, routes, gates, norm_gain,
    expert_gate, expert_up, expert_down, shared_gate, shared_up, shared_down, out_gain,
):
    vmem = pl.BlockSpec(memory_space=pltpu.VMEM)
    hbm = pl.BlockSpec(memory_space=pltpu.HBM)
    dma = pltpu.SemaphoreType.DMA
    buffers = [pltpu.VMEM((4, 4, 4, 16, WIDE), BF), pltpu.VMEM((4, 4, 4, 16, D), BF)]
    buffers += [pltpu.VMEM((3, 4, 4, 16, w), BF) for w in WIDTH]
    buffers += [pltpu.VMEM((4, 4, 16, w), BF) for w in WIDTH]
    buffers += [pltpu.VMEM((3, 4, 16, w), BF) for w in WIDTH]
    buffers += [pltpu.VMEM((4, 16, w), BF) for w in WIDTH]
    buffers += [pltpu.VMEM((3, 16, w), BF) for w in WIDTH]
    buffers += [
        pltpu.VMEM((4, D, 256), BF), pltpu.VMEM((4, D, 256), BF), pltpu.VMEM((4, 256, D), BF),
        pltpu.VMEM((D, 256), BF), pltpu.VMEM((D, 256), BF), pltpu.VMEM((256, D), BF),
        pltpu.VMEM((16, D), F32), pltpu.VMEM((16, 128), F32), pltpu.VMEM((16, 128), F32),
        pltpu.VMEM((256, D), BF), pltpu.VMEM((16, D), F32),
        pltpu.SMEM((4,), jnp.int32), pltpu.VMEM((4, 4, D), BF),
        pltpu.VMEM((4, 4, 8), jnp.int32), pltpu.VMEM((4, 4, 8), F32),
        pltpu.VMEM((1, D), F32), pltpu.VMEM((1, D), F32),
    ]
    return pl.pallas_call(
        kernel,
        out_shape=jax.ShapeDtypeStruct(tokens.shape, BF),
        in_specs=[hbm] * 12,
        out_specs=vmem,
        scratch_shapes=buffers
        + [dma((45,)), dma((45,)), dma((45,)), dma((45,)), dma((3,)), dma((3,)), dma((6,)), dma((6,))],
        compiler_params=pltpu.CompilerParams(
            collective_id=0, has_side_effects=True, vmem_limit_bytes=67043328
        ),
    )(
        lengths, tokens, routes, gates, norm_gain.reshape(1, D), out_gain.reshape(1, D),
        expert_gate, expert_up, expert_down, shared_gate, shared_up, shared_down,
    )


def solution(mesh):
    placed = (
        P("ep", None, None), P("ep"), P("ep", None, None), P("ep", None, None), P(),
        P("ep", None, None), P("ep", None, None), P("ep", None, None), P(), P(), P(), P(),
    )
    return jax.shard_map(
        per_device, mesh=mesh, in_specs=placed, out_specs=P("ep", None, None), check_vma=False
    )
```

```python
import jax
import jax.numpy as jnp
from jax import lax
from jax.experimental import pallas as pl
from jax.experimental.pallas import tpu as pltpu
from jax.sharding import PartitionSpec as P

MESH = pl.DeviceIdType.MESH
EPS = 1e-06
BF = jnp.bfloat16
F32 = jnp.float32
D = 1024
WIDE = 1152
CUT = 384
WIDTH = (384, 384, 256)
ORDER = (0, 1, 3, 2)
REST = slice(1, 4)
ALL = slice(None)


def kernel(
    lengths_hbm, tokens_hbm, routes_hbm, gates_hbm, ng_hbm, og_hbm,
    eg_ref, eu_ref, ed_ref, sg_ref, su_ref, sd_ref,
    out_ref,
    xg, yb, r1a, r1b, r1c, s1a, s1b, s1c, r2a, r2b, r2c, s2a, s2b, s2c, r3a, r3b, r3c,
    wg, wu, wd, sgv, suv, sdv, rows, meta_a, meta_b, hs, total,
    lengths_ref, tokens_ref, routes_ref, gates_ref, ng_ref, og_ref,
    send_sem, recv_sem, w_send, w_recv, w_local, small,
):
    me = lax.axis_index("ep")
    core = lax.rem(me, 2)
    chip = me // 2
    c = (chip // 16, lax.rem(chip // 4, 4), lax.rem(chip, 4))
    stride = (32, 8, 2)
    partner = me + 1 - 2 * core

    peers = [
        [me + (lax.rem(c[dim] + o, 4) - c[dim]) * stride[dim] for o in range(4)]
        for dim in range(3)
    ]

    barrier = pltpu.get_barrier_semaphore()
    pl.semaphore_signal(barrier, inc=1, device_id=(partner,), device_id_type=MESH)
    for dim in range(3):
        for o in (1, 2, 3):
            pl.semaphore_signal(
                barrier, inc=1, device_id=(peers[dim][o],), device_id_type=MESH
            )

    early = []
    for n, (src, dst) in enumerate(
        (
            (tokens_hbm, tokens_ref), (ng_hbm, ng_ref), (routes_hbm, routes_ref),
            (gates_hbm, gates_ref), (lengths_hbm, lengths_ref), (og_hbm, og_ref),
        )
    ):
        copy = pltpu.make_async_copy(src, dst, small.at[n])
        copy.start()
        early.append(copy)
    mine = pl.ds(2 * core, 2)
    local = []
    for n, (src, dst) in enumerate(
        (
            (eg_ref, wg.at[mine]), (eu_ref, wu.at[mine]), (ed_ref, wd.at[mine]),
            (sg_ref, sgv), (su_ref, suv), (sd_ref, sdv),
        )
    ):
        copy = pltpu.make_async_copy(src, dst, w_local.at[n])
        copy.start()
        local.append(copy)

    for copy in early:
        copy.wait()
    row = lax.broadcasted_iota(jnp.int32, (16, 1), 0)
    limit = jnp.zeros((16, 1), jnp.int32)
    for s in range(4):
        limit = jnp.where(row // 4 == s, lengths_ref[s], limit)
        rows[4 * s : 4 * s + 4, :] = tokens_ref[s].astype(F32)
        meta_a[4 * s : 4 * s + 4, 0:8] = routes_ref[s].astype(F32)
        meta_b[4 * s : 4 * s + 4, 0:8] = gates_ref[s]
    live = lax.rem(row, 4) < limit
    values = rows[...]
    mean = jnp.mean(values * values, axis=-1, keepdims=True)
    normed = (values * lax.rsqrt(mean + EPS) * ng_ref[...]).astype(BF)
    lane = lax.broadcasted_iota(jnp.int32, (16, 128), 1)
    ids = jnp.where(live, meta_a[...], -1.0)
    gate = meta_b[...]
    high = gate.astype(BF).astype(F32)
    low = gate - high
    packed = jnp.where(
        lane < 8,
        ids,
        jnp.where(
            lane < 16,
            pltpu.roll(high, 8, 1),
            jnp.where(lane < 24, pltpu.roll(low, 16, 1), 0.0),
        ),
    )
    xg[0, 0, 0, :, 0:D] = normed
    xg[0, 0, 0, :, D:WIDE] = packed.astype(BF)

    pl.semaphore_wait(barrier, 10)

    def swap(n, dst_slot):
        src, dst = ((eg_ref, wg), (eu_ref, wu), (ed_ref, wd))[n]
        return pltpu.make_async_remote_copy(
            src_ref=src, dst_ref=dst.at[dst_slot], send_sem=w_send.at[n],
            recv_sem=w_recv.at[n], device_id=(partner,), device_id_type=MESH,
        )

    theirs = pl.ds(2 - 2 * core, 2)

    copies = {}

    def block(ref, part, i, j, k, width=CUT):
        index = [0, 0, 0]
        index[part], index[(part + 1) % 3], index[(part + 2) % 3] = i, j, k
        return ref.at[index[0], index[1], index[2], :, pl.ds(CUT * part, width)]

    def send(key, src, dst, dim, o):
        n = len(copies)
        copies[key] = pltpu.make_async_remote_copy(
            src_ref=src, dst_ref=dst, send_sem=send_sem.at[n], recv_sem=recv_sem.at[n],
            device_id=(peers[dim % 3][o],), device_id_type=MESH,
        )
        copies[key].start()

    def arrive(*key):
        copies[key].wait_recv()

    near = (1, 3, 2)
    for part in range(3):
        for o in near:
            send(("a0", part, o), block(xg, part, 0, 0, 0), block(xg, part, 4 - o, 0, 0), part, o)
    for part in range(3):
        for o in near:
            send(
                ("a1o", part, o), block(xg, part, 0, 0, 0), block(xg, part, 0, 4 - o, 0), part + 1, o
            )
    for n in range(3):
        swap(n, mine).start()
    for part in range(3):
        for o in near:
            arrive("a0", part, o)
        for o in near:
            send(
                ("a1", part, o), block(xg, part, REST, 0, 0), block(xg, part, REST, 4 - o, 0), part + 1, o
            )
    for part in range(3):
        for o in near:
            send(
                ("a2l", part, o), block(xg, part, ALL, 0, 0), block(xg, part, ALL, 0, 4 - o), part + 2, o
            )
    for q in near:
        arrive("a1o", 2, 4 - q)
        arrive("a1", 2, 4 - q)
        for o in near:
            send(
                ("a2", 2, q, o), block(xg, 2, ALL, q, 0), block(xg, 2, ALL, q, 4 - o), 1, o
            )
    for o in near:
        arrive("a1o", 1, o)
        arrive("a1", 1, o)
    for o in near:
        send(("a2", 1, o), block(xg, 1, ALL, REST, 0), block(xg, 1, ALL, REST, 4 - o), 0, o)
    for o in near:
        arrive("a1o", 0, o)
        arrive("a1", 0, o)
    for k in ORDER:
        for o in near:
            send(("a2", 0, k, o), block(xg, 0, k, REST, 0), block(xg, 0, k, REST, 4 - o), 2, o)

    for copy in local:
        copy.wait()
    own = xg[0, 0, 0, :, 0:D]
    part_g = jnp.dot(own, sgv[...], preferred_element_type=F32)
    part_u = jnp.dot(own, suv[...], preferred_element_type=F32)
    hidden = (part_g / (1.0 + jnp.exp(-part_g)) * part_u).astype(BF)
    total[...] = jnp.dot(hidden, sdv[...], preferred_element_type=F32)

    for n in range(3):
        swap(n, theirs).wait_recv()

    r1, s1 = (r1a, r1b, r1c), (s1a, s1b, s1c)
    r2, s2 = (r2a, r2b, r2c), (s2a, s2b, s2c)
    r3 = (r3a, r3b, r3c)

    def out_block(part, i, j, k):
        return block(yb, part, i, j, k, WIDTH[part])

    wide_lane = lax.broadcasted_iota(jnp.int32, (256, 128), 1)
    for k in ORDER:
        if k == 0:
            for o in near:
                arrive("a2l", 0, o)
                arrive("a2l", 2, o)
        else:
            arrive("a2l", 1, 4 - k)
            arrive("a2", 1, 4 - k)
        for o in near:
            arrive("a2", 0, k, o)
            if k != 0:
                arrive("a2", 2, k, o)
        info = xg[k, :, :, :, D:WIDE].reshape(256, 128).astype(F32)
        weights = pltpu.roll(info, 120, 1) + pltpu.roll(info, 112, 1)
        x = xg[k, :, :, :, 0:D].reshape(256, D)
        for e in range(4):
            name = (4 * chip + e).astype(F32)
            hit = jnp.where((info == name) & (wide_lane < 8), weights, 0.0)
            w = jnp.sum(hit, axis=1, keepdims=True)
            g = jnp.dot(x, wg[e], preferred_element_type=F32)
            u = jnp.dot(x, wu[e], preferred_element_type=F32)
            hs[:, 256 * e : 256 * e + 256] = (g / (1.0 + jnp.exp(-g)) * u * w).astype(BF)
        y = jnp.dot(hs[...], wd[...].reshape(D, D), preferred_element_type=F32)
        yb[k] = y.astype(BF).reshape(4, 4, 16, D)
        for o in near:
            send(("r1", 0, k, o), out_block(0, k, REST, o), r1a.at[o - 1, k, REST], 2, o)
            if k != 0:
                send(("r1", 2, k, o), out_block(2, ALL, k, o), r1c.at[o - 1, k], 1, o)
        if k != 0:
            send(("r1", 1, k), out_block(1, ALL, REST, k), r1b.at[k - 1, :, REST], 0, k)
    for o in near:
        send(("r1l", 0, o), out_block(0, ALL, 0, o), r1a.at[o - 1, :, 0], 2, o)
        send(("r1l", 1, o), out_block(1, ALL, 0, o), r1b.at[o - 1, :, 0], 0, o)
        send(("r1l", 2, o), out_block(2, ALL, 0, o), r1c.at[o - 1, 0], 1, o)

    for k in (1, 3, 2):
        for o in near:
            arrive("r1", 2, k, o)
        acc = yb[k, 0, :, :, 2 * CUT : D].astype(F32)
        for o in (1, 2, 3):
            acc = acc + r1c[o - 1, k].astype(F32)
        s1c[k] = acc.astype(BF)
        send(("r2", 2, k), s1c.at[k, REST], r2c.at[k - 1, REST], 0, k)
    for o in near:
        arrive("r1", 1, o)
    acc = yb[0, :, 1:4, :, CUT : 2 * CUT].astype(F32)
    for o in (1, 2, 3):
        acc = acc + r1b[o - 1, :, 1:4].astype(F32)
    s1b[:, 1:4] = acc.astype(BF)
    for o in near:
        send(("r2", 1, o), s1b.at[REST, o], r2b.at[o - 1, REST], 2, o)
    for o in near:
        for k in ORDER:
            arrive("r1", 0, k, o)
    acc = yb[:, 1:4, 0, :, 0:CUT].astype(F32)
    for o in (1, 2, 3):
        acc = acc + r1a[o - 1, :, 1:4].astype(F32)
    s1a[:, 1:4] = acc.astype(BF)
    for o in near:
        send(("r2", 0, o), s1a.at[REST, o], r2a.at[o - 1, REST], 1, o)
    for o in near:
        send(("r2l", 2, o), s1c.at[o, 0], r2c.at[o - 1, 0], 0, o)
        send(("r2l", 1, o), s1b.at[0, o], r2b.at[o - 1, 0], 2, o)
        send(("r2l", 0, o), s1a.at[0, o], r2a.at[o - 1, 0], 1, o)

    for part in (2, 1, 0):
        for o in near:
            arrive("r1l", part, o)
        if part == 0:
            acc = yb[:, 0, 0, :, 0:CUT].astype(F32)
        elif part == 1:
            acc = yb[0, :, 0, :, CUT : 2 * CUT].astype(F32)
        else:
            acc = yb[0, 0, :, :, 2 * CUT : D].astype(F32)
        for o in (1, 2, 3):
            line = r1c[o - 1, 0] if part == 2 else r1[part][o - 1, :, 0]
            acc = acc + line.astype(F32)
        total[:, CUT * part : CUT * part + WIDTH[part]] += acc[0]
        for o in near:
            arrive("r2", part, o)
        acc = acc[1:4]
        for o in (1, 2, 3):
            acc = acc + r2[part][o - 1, 1:4].astype(F32)
        s2[part][1:4] = acc.astype(BF)
        for o in near:
            send(("r3", part, o), s2[part].at[o], r3[part].at[o - 1], part, o)
    for part in (2, 1, 0):
        for o in near:
            arrive("r2l", part, o)
        acc = r2[part][0, 0].astype(F32)
        for o in (2, 3):
            acc = acc + r2[part][o - 1, 0].astype(F32)
        for o in near:
            arrive("r3", part, o)
        for o in (1, 2, 3):
            acc = acc + r3[part][o - 1].astype(F32)
        total[:, CUT * part : CUT * part + WIDTH[part]] += acc

    summed = total[...]
    mean = jnp.mean(summed * summed, axis=-1, keepdims=True)
    mixed = jnp.where(live, summed * lax.rsqrt(mean + EPS) * og_ref[...], 0.0)
    mixed = mixed.astype(BF)
    for s in range(4):
        out_ref[s] = mixed[4 * s : 4 * s + 4, :]
    for copy in copies.values():
        copy.wait_send()
    for n in range(3):
        swap(n, mine).wait_send()


def per_device(
    tokens, lengths, routes, gates, norm_gain,
    expert_gate, expert_up, expert_down, shared_gate, shared_up, shared_down, out_gain,
):
    vmem = pl.BlockSpec(memory_space=pltpu.VMEM)
    hbm = pl.BlockSpec(memory_space=pltpu.HBM)
    dma = pltpu.SemaphoreType.DMA
    buffers = [pltpu.VMEM((4, 4, 4, 16, WIDE), BF), pltpu.VMEM((4, 4, 4, 16, D), BF)]
    buffers += [pltpu.VMEM((3, 4, 4, 16, w), BF) for w in WIDTH]
    buffers += [pltpu.VMEM((4, 4, 16, w), BF) for w in WIDTH]
    buffers += [pltpu.VMEM((3, 4, 16, w), BF) for w in WIDTH]
    buffers += [pltpu.VMEM((4, 16, w), BF) for w in WIDTH]
    buffers += [pltpu.VMEM((3, 16, w), BF) for w in WIDTH]
    buffers += [
        pltpu.VMEM((4, D, 256), BF), pltpu.VMEM((4, D, 256), BF), pltpu.VMEM((4, 256, D), BF),
        pltpu.VMEM((D, 256), BF), pltpu.VMEM((D, 256), BF), pltpu.VMEM((256, D), BF),
        pltpu.VMEM((16, D), F32), pltpu.VMEM((16, 128), F32), pltpu.VMEM((16, 128), F32),
        pltpu.VMEM((256, D), BF), pltpu.VMEM((16, D), F32),
        pltpu.SMEM((4,), jnp.int32), pltpu.VMEM((4, 4, D), BF),
        pltpu.VMEM((4, 4, 8), jnp.int32), pltpu.VMEM((4, 4, 8), F32),
        pltpu.VMEM((1, D), F32), pltpu.VMEM((1, D), F32),
    ]
    return pl.pallas_call(
        kernel,
        out_shape=jax.ShapeDtypeStruct(tokens.shape, BF),
        in_specs=[hbm] * 12,
        out_specs=vmem,
        scratch_shapes=buffers
        + [dma((120,)), dma((120,)), dma((3,)), dma((3,)), dma((6,)), dma((6,))],
        compiler_params=pltpu.CompilerParams(
            collective_id=0, has_side_effects=True, vmem_limit_bytes=67043328
        ),
    )(
        lengths, tokens, routes, gates, norm_gain.reshape(1, D), out_gain.reshape(1, D),
        expert_gate, expert_up, expert_down, shared_gate, shared_up, shared_down,
    )


def solution(mesh):
    placed = (
        P("ep", None, None), P("ep"), P("ep", None, None), P("ep", None, None), P(),
        P("ep", None, None), P("ep", None, None), P("ep", None, None), P(), P(), P(), P(),
    )
    return jax.shard_map(
        per_device, mesh=mesh, in_specs=placed, out_specs=P("ep", None, None), check_vma=False
    )
```

```python
import jax
import jax.numpy as jnp
from jax import lax
from jax.experimental import pallas as pl
from jax.experimental.pallas import tpu as pltpu
from jax.sharding import PartitionSpec as P

MESH = pl.DeviceIdType.MESH
EPS = 1e-06
BF = jnp.bfloat16
F32 = jnp.float32
D = 1024
WIDE = 1152
CUT = 384
WIDTH = (384, 384, 256)
ORDER = (0, 1, 3, 2)
REST = slice(1, 4)
ALL = slice(None)


def kernel(
    lengths_hbm, tokens_hbm, routes_hbm, gates_hbm, ng_hbm, og_hbm,
    eg_ref, eu_ref, ed_ref, sg_ref, su_ref, sd_ref,
    out_ref,
    xg, yb, r1a, r1b, r1c, s1a, s1b, s1c, r2a, r2b, r2c, s2a, s2b, s2c, r3a, r3b, r3c,
    wg, wu, wd, sgv, suv, sdv, rows, meta_a, meta_b, hs, total,
    lengths_ref, tokens_ref, routes_ref, gates_ref, ng_ref, og_ref,
    send_sem, recv_sem, w_send, w_recv, w_local, small,
):
    me = lax.axis_index("ep")
    core = lax.rem(me, 2)
    chip = me // 2
    c = (chip // 16, lax.rem(chip // 4, 4), lax.rem(chip, 4))
    stride = (32, 8, 2)
    partner = me + 1 - 2 * core

    peers = [
        [me + (lax.rem(c[dim] + o, 4) - c[dim]) * stride[dim] for o in range(4)]
        for dim in range(3)
    ]

    barrier = pltpu.get_barrier_semaphore()
    pl.semaphore_signal(barrier, inc=1, device_id=(partner,), device_id_type=MESH)
    for dim in range(3):
        for o in (1, 2, 3):
            pl.semaphore_signal(
                barrier, inc=1, device_id=(peers[dim][o],), device_id_type=MESH
            )

    early = []
    for n, (src, dst) in enumerate(
        (
            (tokens_hbm, tokens_ref), (ng_hbm, ng_ref), (routes_hbm, routes_ref),
            (gates_hbm, gates_ref), (lengths_hbm, lengths_ref), (og_hbm, og_ref),
        )
    ):
        copy = pltpu.make_async_copy(src, dst, small.at[n])
        copy.start()
        early.append(copy)
    mine = pl.ds(2 * core, 2)
    local = []
    for n, (src, dst) in enumerate(
        (
            (eg_ref, wg.at[mine]), (eu_ref, wu.at[mine]), (ed_ref, wd.at[mine]),
            (sg_ref, sgv), (su_ref, suv), (sd_ref, sdv),
        )
    ):
        copy = pltpu.make_async_copy(src, dst, w_local.at[n])
        copy.start()
        local.append(copy)

    for copy in early:
        copy.wait()
    row = lax.broadcasted_iota(jnp.int32, (16, 1), 0)
    limit = jnp.zeros((16, 1), jnp.int32)
    for s in range(4):
        limit = jnp.where(row // 4 == s, lengths_ref[s], limit)
        rows[4 * s : 4 * s + 4, :] = tokens_ref[s].astype(F32)
        meta_a[4 * s : 4 * s + 4, 0:8] = routes_ref[s].astype(F32)
        meta_b[4 * s : 4 * s + 4, 0:8] = gates_ref[s]
    live = lax.rem(row, 4) < limit
    values = rows[...]
    mean = jnp.mean(values * values, axis=-1, keepdims=True)
    normed = (values * lax.rsqrt(mean + EPS) * ng_ref[...]).astype(BF)
    lane = lax.broadcasted_iota(jnp.int32, (16, 128), 1)
    ids = jnp.where(live, meta_a[...], -1.0)
    gate = meta_b[...]
    high = gate.astype(BF).astype(F32)
    low = gate - high
    packed = jnp.where(
        lane < 8,
        ids,
        jnp.where(
            lane < 16,
            pltpu.roll(high, 8, 1),
            jnp.where(lane < 24, pltpu.roll(low, 16, 1), 0.0),
        ),
    )
    xg[0, 0, 0, :, 0:D] = normed
    xg[0, 0, 0, :, D:WIDE] = packed.astype(BF)

    pl.semaphore_wait(barrier, 10)

    def swap(n, dst_slot):
        src, dst = ((eg_ref, wg), (eu_ref, wu), (ed_ref, wd))[n]
        return pltpu.make_async_remote_copy(
            src_ref=src, dst_ref=dst.at[dst_slot], send_sem=w_send.at[n],
            recv_sem=w_recv.at[n], device_id=(partner,), device_id_type=MESH,
        )

    theirs = pl.ds(2 - 2 * core, 2)

    copies = {}

    def block(ref, part, i, j, k, width=CUT):
        index = [0, 0, 0]
        index[part], index[(part + 1) % 3], index[(part + 2) % 3] = i, j, k
        return ref.at[index[0], index[1], index[2], :, pl.ds(CUT * part, width)]

    def send(key, src, dst, dim, o):
        n = len(copies)
        copies[key] = pltpu.make_async_remote_copy(
            src_ref=src, dst_ref=dst, send_sem=send_sem.at[n], recv_sem=recv_sem.at[n],
            device_id=(peers[dim % 3][o],), device_id_type=MESH,
        )
        copies[key].start()

    def arrive(*key):
        copies[key].wait_recv()

    near = (1, 3, 2)
    for part in range(3):
        for o in near:
            send(("a0", part, o), block(xg, part, 0, 0, 0), block(xg, part, 4 - o, 0, 0), part, o)
    for part in range(3):
        for o in near:
            send(
                ("a1o", part, o), block(xg, part, 0, 0, 0), block(xg, part, 0, 4 - o, 0), part + 1, o
            )
    for n in range(3):
        swap(n, mine).start()
    for part in range(3):
        for o in near:
            arrive("a0", part, o)
        for o in near:
            send(
                ("a1", part, o), block(xg, part, REST, 0, 0), block(xg, part, REST, 4 - o, 0), part + 1, o
            )
    for part in range(3):
        for o in near:
            send(
                ("a2l", part, o), block(xg, part, ALL, 0, 0), block(xg, part, ALL, 0, 4 - o), part + 2, o
            )
    for o in near:
        arrive("a1o", 0, o)
        arrive("a1", 0, o)
    for k in ORDER:
        for o in near:
            send(("a2", 0, k, o), block(xg, 0, k, REST, 0), block(xg, 0, k, REST, 4 - o), 2, o)
    for o in near:
        arrive("a1o", 1, o)
        arrive("a1", 1, o)
    for o in near:
        send(("a2", 1, o), block(xg, 1, ALL, REST, 0), block(xg, 1, ALL, REST, 4 - o), 0, o)
    for q in near:
        arrive("a1o", 2, 4 - q)
        arrive("a1", 2, 4 - q)
        for o in near:
            send(("a2", 2, q, o), block(xg, 2, ALL, q, 0), block(xg, 2, ALL, q, 4 - o), 1, o)

    for copy in local:
        copy.wait()
    own = xg[0, 0, 0, :, 0:D]
    part_g = jnp.dot(own, sgv[...], preferred_element_type=F32)
    part_u = jnp.dot(own, suv[...], preferred_element_type=F32)
    hidden = (part_g / (1.0 + jnp.exp(-part_g)) * part_u).astype(BF)
    total[...] = jnp.dot(hidden, sdv[...], preferred_element_type=F32)

    for n in range(3):
        swap(n, theirs).wait_recv()

    r1, s1 = (r1a, r1b, r1c), (s1a, s1b, s1c)
    r2, s2 = (r2a, r2b, r2c), (s2a, s2b, s2c)
    r3 = (r3a, r3b, r3c)

    def out_block(part, i, j, k):
        return block(yb, part, i, j, k, WIDTH[part])

    wide_lane = lax.broadcasted_iota(jnp.int32, (256, 128), 1)
    for k in ORDER:
        if k == 0:
            for o in near:
                arrive("a2l", 0, o)
                arrive("a2l", 2, o)
        else:
            arrive("a2l", 1, 4 - k)
            arrive("a2", 1, 4 - k)
        for o in near:
            arrive("a2", 0, k, o)
            if k != 0:
                arrive("a2", 2, k, o)
        info = xg[k, :, :, :, D:WIDE].reshape(256, 128).astype(F32)
        weights = pltpu.roll(info, 120, 1) + pltpu.roll(info, 112, 1)
        x = xg[k, :, :, :, 0:D].reshape(256, D)
        for e in range(4):
            name = (4 * chip + e).astype(F32)
            hit = jnp.where((info == name) & (wide_lane < 8), weights, 0.0)
            w = jnp.sum(hit, axis=1, keepdims=True)
            g = jnp.dot(x, wg[e], preferred_element_type=F32)
            u = jnp.dot(x, wu[e], preferred_element_type=F32)
            hs[:, 256 * e : 256 * e + 256] = (g / (1.0 + jnp.exp(-g)) * u * w).astype(BF)
        y = jnp.dot(hs[...], wd[...].reshape(D, D), preferred_element_type=F32)
        yb[k] = y.astype(BF).reshape(4, 4, 16, D)
        for o in near:
            send(("r1", 0, k, o), out_block(0, k, REST, o), r1a.at[o - 1, k, REST], 2, o)
            if k != 0:
                send(("r1", 2, k, o), out_block(2, ALL, k, o), r1c.at[o - 1, k], 1, o)
        if k != 0:
            send(("r1", 1, k), out_block(1, ALL, REST, k), r1b.at[k - 1, :, REST], 0, k)
    for o in near:
        send(("r1l", 0, o), out_block(0, ALL, 0, o), r1a.at[o - 1, :, 0], 2, o)
        send(("r1l", 1, o), out_block(1, ALL, 0, o), r1b.at[o - 1, :, 0], 0, o)
        send(("r1l", 2, o), out_block(2, ALL, 0, o), r1c.at[o - 1, 0], 1, o)

    for k in (1, 3, 2):
        for o in near:
            arrive("r1", 2, k, o)
        acc = yb[k, 0, :, :, 2 * CUT : D].astype(F32)
        for o in (1, 2, 3):
            acc = acc + r1c[o - 1, k].astype(F32)
        s1c[k] = acc.astype(BF)
        send(("r2", 2, k), s1c.at[k, REST], r2c.at[k - 1, REST], 0, k)
    for o in near:
        arrive("r1", 1, o)
    acc = yb[0, :, 1:4, :, CUT : 2 * CUT].astype(F32)
    for o in (1, 2, 3):
        acc = acc + r1b[o - 1, :, 1:4].astype(F32)
    s1b[:, 1:4] = acc.astype(BF)
    for o in near:
        send(("r2", 1, o), s1b.at[REST, o], r2b.at[o - 1, REST], 2, o)
    for o in near:
        for k in ORDER:
            arrive("r1", 0, k, o)
    acc = yb[:, 1:4, 0, :, 0:CUT].astype(F32)
    for o in (1, 2, 3):
        acc = acc + r1a[o - 1, :, 1:4].astype(F32)
    s1a[:, 1:4] = acc.astype(BF)
    for o in near:
        send(("r2", 0, o), s1a.at[REST, o], r2a.at[o - 1, REST], 1, o)
    for o in near:
        send(("r2l", 2, o), s1c.at[o, 0], r2c.at[o - 1, 0], 0, o)
        send(("r2l", 1, o), s1b.at[0, o], r2b.at[o - 1, 0], 2, o)
        send(("r2l", 0, o), s1a.at[0, o], r2a.at[o - 1, 0], 1, o)

    for part in (2, 1, 0):
        for o in near:
            arrive("r1l", part, o)
        if part == 0:
            acc = yb[:, 0, 0, :, 0:CUT].astype(F32)
        elif part == 1:
            acc = yb[0, :, 0, :, CUT : 2 * CUT].astype(F32)
        else:
            acc = yb[0, 0, :, :, 2 * CUT : D].astype(F32)
        for o in (1, 2, 3):
            line = r1c[o - 1, 0] if part == 2 else r1[part][o - 1, :, 0]
            acc = acc + line.astype(F32)
        total[:, CUT * part : CUT * part + WIDTH[part]] += acc[0]
        for o in near:
            arrive("r2", part, o)
        acc = acc[1:4]
        for o in (1, 2, 3):
            acc = acc + r2[part][o - 1, 1:4].astype(F32)
        s2[part][1:4] = acc.astype(BF)
        for o in near:
            send(("r3", part, o), s2[part].at[o], r3[part].at[o - 1], part, o)
    for part in (2, 1, 0):
        for o in near:
            arrive("r2l", part, o)
        acc = r2[part][0, 0].astype(F32)
        for o in (2, 3):
            acc = acc + r2[part][o - 1, 0].astype(F32)
        for o in near:
            arrive("r3", part, o)
        for o in (1, 2, 3):
            acc = acc + r3[part][o - 1].astype(F32)
        total[:, CUT * part : CUT * part + WIDTH[part]] += acc

    summed = total[...]
    mean = jnp.mean(summed * summed, axis=-1, keepdims=True)
    mixed = jnp.where(live, summed * lax.rsqrt(mean + EPS) * og_ref[...], 0.0)
    mixed = mixed.astype(BF)
    for s in range(4):
        out_ref[s] = mixed[4 * s : 4 * s + 4, :]
    for copy in copies.values():
        copy.wait_send()
    for n in range(3):
        swap(n, mine).wait_send()


def per_device(
    tokens, lengths, routes, gates, norm_gain,
    expert_gate, expert_up, expert_down, shared_gate, shared_up, shared_down, out_gain,
):
    vmem = pl.BlockSpec(memory_space=pltpu.VMEM)
    hbm = pl.BlockSpec(memory_space=pltpu.HBM)
    dma = pltpu.SemaphoreType.DMA
    buffers = [pltpu.VMEM((4, 4, 4, 16, WIDE), BF), pltpu.VMEM((4, 4, 4, 16, D), BF)]
    buffers += [pltpu.VMEM((3, 4, 4, 16, w), BF) for w in WIDTH]
    buffers += [pltpu.VMEM((4, 4, 16, w), BF) for w in WIDTH]
    buffers += [pltpu.VMEM((3, 4, 16, w), BF) for w in WIDTH]
    buffers += [pltpu.VMEM((4, 16, w), BF) for w in WIDTH]
    buffers += [pltpu.VMEM((3, 16, w), BF) for w in WIDTH]
    buffers += [
        pltpu.VMEM((4, D, 256), BF), pltpu.VMEM((4, D, 256), BF), pltpu.VMEM((4, 256, D), BF),
        pltpu.VMEM((D, 256), BF), pltpu.VMEM((D, 256), BF), pltpu.VMEM((256, D), BF),
        pltpu.VMEM((16, D), F32), pltpu.VMEM((16, 128), F32), pltpu.VMEM((16, 128), F32),
        pltpu.VMEM((256, D), BF), pltpu.VMEM((16, D), F32),
        pltpu.SMEM((4,), jnp.int32), pltpu.VMEM((4, 4, D), BF),
        pltpu.VMEM((4, 4, 8), jnp.int32), pltpu.VMEM((4, 4, 8), F32),
        pltpu.VMEM((1, D), F32), pltpu.VMEM((1, D), F32),
    ]
    return pl.pallas_call(
        kernel,
        out_shape=jax.ShapeDtypeStruct(tokens.shape, BF),
        in_specs=[hbm] * 12,
        out_specs=vmem,
        scratch_shapes=buffers
        + [dma((120,)), dma((120,)), dma((3,)), dma((3,)), dma((6,)), dma((6,))],
        compiler_params=pltpu.CompilerParams(
            collective_id=0, has_side_effects=True, vmem_limit_bytes=67043328
        ),
    )(
        lengths, tokens, routes, gates, norm_gain.reshape(1, D), out_gain.reshape(1, D),
        expert_gate, expert_up, expert_down, shared_gate, shared_up, shared_down,
    )


def solution(mesh):
    placed = (
        P("ep", None, None), P("ep"), P("ep", None, None), P("ep", None, None), P(),
        P("ep", None, None), P("ep", None, None), P("ep", None, None), P(), P(), P(), P(),
    )
    return jax.shard_map(
        per_device, mesh=mesh, in_specs=placed, out_specs=P("ep", None, None), check_vma=False
    )
```

```python
import jax
import jax.numpy as jnp
from jax import lax
from jax.experimental import pallas as pl
from jax.experimental.pallas import tpu as pltpu
from jax.sharding import PartitionSpec as P

MESH = pl.DeviceIdType.MESH
EPS = 1e-06
BF = jnp.bfloat16
F32 = jnp.float32
D = 1024
WIDE = 1152
CUT = 384
WIDTH = (384, 384, 256)
ORDER = (0, 1, 3, 2)
REST = slice(1, 4)
ALL = slice(None)


def kernel(
    lengths_hbm, tokens_hbm, routes_hbm, gates_hbm, ng_hbm, og_hbm,
    eg_ref, eu_ref, ed_ref, sg_ref, su_ref, sd_ref,
    out_ref,
    xg, yb, r1a, r1b, r1c, s1a, s1b, s1c, r2a, r2b, r2c, s2a, s2b, s2c, r3a, r3b, r3c,
    wg, wu, wd, sgv, suv, sdv, rows, meta_a, meta_b, hs, total,
    lengths_ref, tokens_ref, routes_ref, gates_ref, ng_ref, og_ref,
    send_sem, recv_sem, w_send, w_recv, w_local, small,
):
    me = lax.axis_index("ep")
    core = lax.rem(me, 2)
    chip = me // 2
    c = (chip // 16, lax.rem(chip // 4, 4), lax.rem(chip, 4))
    stride = (32, 8, 2)
    partner = me + 1 - 2 * core

    peers = [
        [me + (lax.rem(c[dim] + o, 4) - c[dim]) * stride[dim] for o in range(4)]
        for dim in range(3)
    ]

    barrier = pltpu.get_barrier_semaphore()
    pl.semaphore_signal(barrier, inc=1, device_id=(partner,), device_id_type=MESH)
    for dim in range(3):
        for o in (1, 2, 3):
            pl.semaphore_signal(
                barrier, inc=1, device_id=(peers[dim][o],), device_id_type=MESH
            )

    early = []
    for n, (src, dst) in enumerate(
        (
            (tokens_hbm, tokens_ref), (ng_hbm, ng_ref), (routes_hbm, routes_ref),
            (gates_hbm, gates_ref), (lengths_hbm, lengths_ref), (og_hbm, og_ref),
        )
    ):
        copy = pltpu.make_async_copy(src, dst, small.at[n])
        copy.start()
        early.append(copy)
    mine = pl.ds(2 * core, 2)
    local = []
    for n, (src, dst) in enumerate(
        (
            (eg_ref, wg.at[mine]), (eu_ref, wu.at[mine]), (ed_ref, wd.at[mine]),
            (sg_ref, sgv), (su_ref, suv), (sd_ref, sdv),
        )
    ):
        copy = pltpu.make_async_copy(src, dst, w_local.at[n])
        copy.start()
        local.append(copy)

    for copy in early:
        copy.wait()
    row = lax.broadcasted_iota(jnp.int32, (16, 1), 0)
    limit = jnp.zeros((16, 1), jnp.int32)
    for s in range(4):
        limit = jnp.where(row // 4 == s, lengths_ref[s], limit)
        rows[4 * s : 4 * s + 4, :] = tokens_ref[s].astype(F32)
        meta_a[4 * s : 4 * s + 4, 0:8] = routes_ref[s].astype(F32)
        meta_b[4 * s : 4 * s + 4, 0:8] = gates_ref[s]
    live = lax.rem(row, 4) < limit
    values = rows[...]
    mean = jnp.mean(values * values, axis=-1, keepdims=True)
    normed = (values * lax.rsqrt(mean + EPS) * ng_ref[...]).astype(BF)
    xg[0, 0, 0, :, 0:D] = normed

    pl.semaphore_wait(barrier, 10)

    def swap(n, dst_slot):
        src, dst = ((eg_ref, wg), (eu_ref, wu), (ed_ref, wd))[n]
        return pltpu.make_async_remote_copy(
            src_ref=src, dst_ref=dst.at[dst_slot], send_sem=w_send.at[n],
            recv_sem=w_recv.at[n], device_id=(partner,), device_id_type=MESH,
        )

    theirs = pl.ds(2 - 2 * core, 2)

    copies = {}

    def block(ref, part, i, j, k, width=CUT):
        index = [0, 0, 0]
        index[part], index[(part + 1) % 3], index[(part + 2) % 3] = i, j, k
        return ref.at[index[0], index[1], index[2], :, pl.ds(CUT * part, width)]

    def send(key, src, dst, dim, o):
        n = len(copies)
        copies[key] = pltpu.make_async_remote_copy(
            src_ref=src, dst_ref=dst, send_sem=send_sem.at[n], recv_sem=recv_sem.at[n],
            device_id=(peers[dim % 3][o],), device_id_type=MESH,
        )
        copies[key].start()

    def arrive(*key):
        copies[key].wait_recv()

    def drain(*kinds):
        for key in copies:
            if key[0] in kinds:
                copies[key].wait_send()

    near = (1, 3, 2)
    for part in range(3):
        if part == 2:
            lane = lax.broadcasted_iota(jnp.int32, (16, 128), 1)
            ids = jnp.where(live, meta_a[...], -1.0)
            gate = meta_b[...]
            high = gate.astype(BF).astype(F32)
            low = gate - high
            packed = jnp.where(
                lane < 8,
                ids,
                jnp.where(
                    lane < 16,
                    pltpu.roll(high, 8, 1),
                    jnp.where(lane < 24, pltpu.roll(low, 16, 1), 0.0),
                ),
            )
            xg[0, 0, 0, :, D:WIDE] = packed.astype(BF)
        for o in near:
            send(("a0", part, o), block(xg, part, 0, 0, 0), block(xg, part, 4 - o, 0, 0), part, o)
    for part in range(3):
        for o in near:
            send(
                ("a1o", part, o), block(xg, part, 0, 0, 0), block(xg, part, 0, 4 - o, 0), part + 1, o
            )
    for n in range(3):
        swap(n, mine).start()
    for part in range(3):
        for o in near:
            arrive("a0", part, o)
        for o in near:
            send(
                ("a1", part, o), block(xg, part, REST, 0, 0), block(xg, part, REST, 4 - o, 0), part + 1, o
            )
    for part in range(3):
        for o in near:
            send(
                ("a2l", part, o), block(xg, part, ALL, 0, 0), block(xg, part, ALL, 0, 4 - o), part + 2, o
            )
    for o in near:
        arrive("a1o", 0, o)
        arrive("a1", 0, o)
    for k in ORDER:
        for o in near:
            send(("a2", 0, k, o), block(xg, 0, k, REST, 0), block(xg, 0, k, REST, 4 - o), 2, o)
    for o in near:
        arrive("a1o", 1, o)
        arrive("a1", 1, o)
    for o in near:
        send(("a2", 1, o), block(xg, 1, ALL, REST, 0), block(xg, 1, ALL, REST, 4 - o), 0, o)
    for q in near:
        arrive("a1o", 2, 4 - q)
        arrive("a1", 2, 4 - q)
        for o in near:
            send(("a2", 2, q, o), block(xg, 2, ALL, q, 0), block(xg, 2, ALL, q, 4 - o), 1, o)

    for copy in local:
        copy.wait()
    own = xg[0, 0, 0, :, 0:D]
    part_g = jnp.dot(own, sgv[...], preferred_element_type=F32)
    part_u = jnp.dot(own, suv[...], preferred_element_type=F32)
    hidden = (part_g / (1.0 + jnp.exp(-part_g)) * part_u).astype(BF)
    total[...] = jnp.dot(hidden, sdv[...], preferred_element_type=F32)

    for n in range(3):
        swap(n, theirs).wait_recv()

    r1, s1 = (r1a, r1b, r1c), (s1a, s1b, s1c)
    r2, s2 = (r2a, r2b, r2c), (s2a, s2b, s2c)
    r3 = (r3a, r3b, r3c)

    def out_block(part, i, j, k):
        return block(yb, part, i, j, k, WIDTH[part])

    wide_lane = lax.broadcasted_iota(jnp.int32, (256, 128), 1)
    for k in ORDER:
        if k == 0:
            for o in near:
                arrive("a2l", 0, o)
                arrive("a2l", 2, o)
        else:
            arrive("a2l", 1, 4 - k)
            arrive("a2", 1, 4 - k)
        for o in near:
            arrive("a2", 0, k, o)
            if k != 0:
                arrive("a2", 2, k, o)
        info = xg[k, :, :, :, D:WIDE].reshape(256, 128).astype(F32)
        weights = pltpu.roll(info, 120, 1) + pltpu.roll(info, 112, 1)
        x = xg[k, :, :, :, 0:D].reshape(256, D)
        for e in range(4):
            name = (4 * chip + e).astype(F32)
            hit = jnp.where((info == name) & (wide_lane < 8), weights, 0.0)
            w = jnp.sum(hit, axis=1, keepdims=True)
            g = jnp.dot(x, wg[e], preferred_element_type=F32)
            u = jnp.dot(x, wu[e], preferred_element_type=F32)
            hs[:, 256 * e : 256 * e + 256] = (g / (1.0 + jnp.exp(-g)) * u * w).astype(BF)
        y = jnp.dot(hs[...], wd[...].reshape(D, D), preferred_element_type=F32)
        yb[k] = y.astype(BF).reshape(4, 4, 16, D)
        for o in near:
            send(("r1", 0, k, o), out_block(0, k, REST, o), r1a.at[o - 1, k, REST], 2, o)
            if k != 0:
                send(("r1", 2, k, o), out_block(2, ALL, k, o), r1c.at[o - 1, k], 1, o)
        if k != 0:
            send(("r1", 1, k), out_block(1, ALL, REST, k), r1b.at[k - 1, :, REST], 0, k)
    for o in near:
        send(("r1l", 0, o), out_block(0, ALL, 0, o), r1a.at[o - 1, :, 0], 2, o)
        send(("r1l", 1, o), out_block(1, ALL, 0, o), r1b.at[o - 1, :, 0], 0, o)
        send(("r1l", 2, o), out_block(2, ALL, 0, o), r1c.at[o - 1, 0], 1, o)

    for k in (1, 3, 2):
        for o in near:
            arrive("r1", 2, k, o)
        acc = yb[k, 0, :, :, 2 * CUT : D].astype(F32)
        for o in (1, 2, 3):
            acc = acc + r1c[o - 1, k].astype(F32)
        s1c[k] = acc.astype(BF)
        send(("r2", 2, k), s1c.at[k, REST], r2c.at[k - 1, REST], 0, k)
    for o in near:
        arrive("r1", 1, o)
    acc = yb[0, :, 1:4, :, CUT : 2 * CUT].astype(F32)
    for o in (1, 2, 3):
        acc = acc + r1b[o - 1, :, 1:4].astype(F32)
    s1b[:, 1:4] = acc.astype(BF)
    for o in near:
        send(("r2", 1, o), s1b.at[REST, o], r2b.at[o - 1, REST], 2, o)
    for o in near:
        for k in ORDER:
            arrive("r1", 0, k, o)
    acc = yb[:, 1:4, 0, :, 0:CUT].astype(F32)
    for o in (1, 2, 3):
        acc = acc + r1a[o - 1, :, 1:4].astype(F32)
    s1a[:, 1:4] = acc.astype(BF)
    for o in near:
        send(("r2", 0, o), s1a.at[REST, o], r2a.at[o - 1, REST], 1, o)
    for o in near:
        send(("r2l", 2, o), s1c.at[o, 0], r2c.at[o - 1, 0], 0, o)
        send(("r2l", 1, o), s1b.at[0, o], r2b.at[o - 1, 0], 2, o)
        send(("r2l", 0, o), s1a.at[0, o], r2a.at[o - 1, 0], 1, o)

    drain("a0", "a1o", "a1", "a2l", "a2")
    for n in range(3):
        swap(n, mine).wait_send()

    for part in (2, 1, 0):
        for o in near:
            arrive("r1l", part, o)
        if part == 0:
            acc = yb[:, 0, 0, :, 0:CUT].astype(F32)
        elif part == 1:
            acc = yb[0, :, 0, :, CUT : 2 * CUT].astype(F32)
        else:
            acc = yb[0, 0, :, :, 2 * CUT : D].astype(F32)
        for o in (1, 2, 3):
            line = r1c[o - 1, 0] if part == 2 else r1[part][o - 1, :, 0]
            acc = acc + line.astype(F32)
        total[:, CUT * part : CUT * part + WIDTH[part]] += acc[0]
        for o in near:
            arrive("r2", part, o)
        acc = acc[1:4]
        for o in (1, 2, 3):
            acc = acc + r2[part][o - 1, 1:4].astype(F32)
        s2[part][1:4] = acc.astype(BF)
        for o in near:
            send(("r3", part, o), s2[part].at[o], r3[part].at[o - 1], part, o)
    drain("r1", "r1l", "r2", "r2l")
    for part in (2, 1, 0):
        for o in near:
            arrive("r2l", part, o)
        acc = r2[part][0, 0].astype(F32)
        for o in (2, 3):
            acc = acc + r2[part][o - 1, 0].astype(F32)
        for o in near:
            arrive("r3", part, o)
        for o in (1, 2, 3):
            acc = acc + r3[part][o - 1].astype(F32)
        total[:, CUT * part : CUT * part + WIDTH[part]] += acc

    summed = total[...]
    mean = jnp.mean(summed * summed, axis=-1, keepdims=True)
    mixed = jnp.where(live, summed * lax.rsqrt(mean + EPS) * og_ref[...], 0.0)
    mixed = mixed.astype(BF)
    for s in range(4):
        out_ref[s] = mixed[4 * s : 4 * s + 4, :]
    drain("r3")


def per_device(
    tokens, lengths, routes, gates, norm_gain,
    expert_gate, expert_up, expert_down, shared_gate, shared_up, shared_down, out_gain,
):
    vmem = pl.BlockSpec(memory_space=pltpu.VMEM)
    hbm = pl.BlockSpec(memory_space=pltpu.HBM)
    dma = pltpu.SemaphoreType.DMA
    buffers = [pltpu.VMEM((4, 4, 4, 16, WIDE), BF), pltpu.VMEM((4, 4, 4, 16, D), BF)]
    buffers += [pltpu.VMEM((3, 4, 4, 16, w), BF) for w in WIDTH]
    buffers += [pltpu.VMEM((4, 4, 16, w), BF) for w in WIDTH]
    buffers += [pltpu.VMEM((3, 4, 16, w), BF) for w in WIDTH]
    buffers += [pltpu.VMEM((4, 16, w), BF) for w in WIDTH]
    buffers += [pltpu.VMEM((3, 16, w), BF) for w in WIDTH]
    buffers += [
        pltpu.VMEM((4, D, 256), BF), pltpu.VMEM((4, D, 256), BF), pltpu.VMEM((4, 256, D), BF),
        pltpu.VMEM((D, 256), BF), pltpu.VMEM((D, 256), BF), pltpu.VMEM((256, D), BF),
        pltpu.VMEM((16, D), F32), pltpu.VMEM((16, 128), F32), pltpu.VMEM((16, 128), F32),
        pltpu.VMEM((256, D), BF), pltpu.VMEM((16, D), F32),
        pltpu.SMEM((4,), jnp.int32), pltpu.VMEM((4, 4, D), BF),
        pltpu.VMEM((4, 4, 8), jnp.int32), pltpu.VMEM((4, 4, 8), F32),
        pltpu.VMEM((1, D), F32), pltpu.VMEM((1, D), F32),
    ]
    return pl.pallas_call(
        kernel,
        out_shape=jax.ShapeDtypeStruct(tokens.shape, BF),
        in_specs=[hbm] * 12,
        out_specs=vmem,
        scratch_shapes=buffers
        + [dma((120,)), dma((120,)), dma((3,)), dma((3,)), dma((6,)), dma((6,))],
        compiler_params=pltpu.CompilerParams(
            collective_id=0, has_side_effects=True, vmem_limit_bytes=67043328
        ),
    )(
        lengths, tokens, routes, gates, norm_gain.reshape(1, D), out_gain.reshape(1, D),
        expert_gate, expert_up, expert_down, shared_gate, shared_up, shared_down,
    )


def solution(mesh):
    placed = (
        P("ep", None, None), P("ep"), P("ep", None, None), P("ep", None, None), P(),
        P("ep", None, None), P("ep", None, None), P("ep", None, None), P(), P(), P(), P(),
    )
    return jax.shard_map(
        per_device, mesh=mesh, in_specs=placed, out_specs=P("ep", None, None), check_vma=False
    )
```

```python
import jax
import jax.numpy as jnp
from jax import lax
from jax.experimental import pallas as pl
from jax.experimental.pallas import tpu as pltpu
from jax.sharding import PartitionSpec as P

MESH = pl.DeviceIdType.MESH
EPS = 1e-06
BF = jnp.bfloat16
F32 = jnp.float32
D = 1024
WIDE = 1152
CUT = 384
WIDTH = (384, 384, 256)
ORDER = (0, 1, 3, 2)
REST = slice(1, 4)
ALL = slice(None)


def kernel(
    lengths_hbm, tokens_hbm, routes_hbm, gates_hbm, ng_hbm, og_hbm,
    eg_ref, eu_ref, ed_ref, sg_ref, su_ref, sd_ref,
    out_ref,
    xg, yb, r1a, r1b, r1c, s1a, s1b, s1c, r2a, r2b, r2c, s2a, s2b, s2c, r3a, r3b, r3c,
    wg, wu, wd, sgv, suv, sdv, rows, meta_a, meta_b, hs, total,
    lengths_ref, tokens_ref, routes_ref, gates_ref, ng_ref, og_ref,
    send_sem, recv_sem, w_send, w_recv, w_local, small,
):
    me = lax.axis_index("ep")
    core = lax.rem(me, 2)
    chip = me // 2
    c = (chip // 16, lax.rem(chip // 4, 4), lax.rem(chip, 4))
    stride = (32, 8, 2)
    partner = me + 1 - 2 * core

    peers = [
        [me + (lax.rem(c[dim] + o, 4) - c[dim]) * stride[dim] for o in range(4)]
        for dim in range(3)
    ]

    barrier = pltpu.get_barrier_semaphore()
    pl.semaphore_signal(barrier, inc=1, device_id=(partner,), device_id_type=MESH)
    for dim in range(3):
        for o in (1, 2, 3):
            pl.semaphore_signal(
                barrier, inc=1, device_id=(peers[dim][o],), device_id_type=MESH
            )

    early = []
    for n, (src, dst) in enumerate(
        (
            (tokens_hbm, tokens_ref), (ng_hbm, ng_ref), (routes_hbm, routes_ref),
            (gates_hbm, gates_ref), (lengths_hbm, lengths_ref), (og_hbm, og_ref),
        )
    ):
        copy = pltpu.make_async_copy(src, dst, small.at[n])
        copy.start()
        early.append(copy)
    mine = pl.ds(2 * core, 2)
    row = lax.broadcasted_iota(jnp.int32, (16, 1), 0)
    early[0].wait()
    early[1].wait()
    for s in range(4):
        rows[4 * s : 4 * s + 4, :] = tokens_ref[s].astype(F32)
    values = rows[...]
    mean = jnp.mean(values * values, axis=-1, keepdims=True)
    normed = (values * lax.rsqrt(mean + EPS) * ng_ref[...]).astype(BF)
    xg[0, 0, 0, :, 0:D] = normed

    for copy in early[2:]:
        copy.wait()
    limit = jnp.zeros((16, 1), jnp.int32)
    for s in range(4):
        limit = jnp.where(row // 4 == s, lengths_ref[s], limit)
        meta_a[4 * s : 4 * s + 4, 0:8] = routes_ref[s].astype(F32)
        meta_b[4 * s : 4 * s + 4, 0:8] = gates_ref[s]
    live = lax.rem(row, 4) < limit
    pl.semaphore_wait(barrier, 10)

    def swap(n, dst_slot):
        src, dst = ((eg_ref, wg), (eu_ref, wu), (ed_ref, wd))[n]
        return pltpu.make_async_remote_copy(
            src_ref=src, dst_ref=dst.at[dst_slot], send_sem=w_send.at[n],
            recv_sem=w_recv.at[n], device_id=(partner,), device_id_type=MESH,
        )

    theirs = pl.ds(2 - 2 * core, 2)

    copies = {}

    def block(ref, part, i, j, k, width=CUT):
        index = [0, 0, 0]
        index[part], index[(part + 1) % 3], index[(part + 2) % 3] = i, j, k
        return ref.at[index[0], index[1], index[2], :, pl.ds(CUT * part, width)]

    def send(key, src, dst, dim, o):
        n = len(copies)
        copies[key] = pltpu.make_async_remote_copy(
            src_ref=src, dst_ref=dst, send_sem=send_sem.at[n], recv_sem=recv_sem.at[n],
            device_id=(peers[dim % 3][o],), device_id_type=MESH,
        )
        copies[key].start()

    def arrive(*key):
        copies[key].wait_recv()

    def drain(*kinds):
        for key in copies:
            if key[0] in kinds:
                copies[key].wait_send()

    near = (1, 3, 2)
    for part in range(3):
        if part == 2:
            lane = lax.broadcasted_iota(jnp.int32, (16, 128), 1)
            ids = jnp.where(live, meta_a[...], -1.0)
            gate = meta_b[...]
            high = gate.astype(BF).astype(F32)
            low = gate - high
            packed = jnp.where(
                lane < 8,
                ids,
                jnp.where(
                    lane < 16,
                    pltpu.roll(high, 8, 1),
                    jnp.where(lane < 24, pltpu.roll(low, 16, 1), 0.0),
                ),
            )
            xg[0, 0, 0, :, D:WIDE] = packed.astype(BF)
        for o in near:
            send(("a0", part, o), block(xg, part, 0, 0, 0), block(xg, part, 4 - o, 0, 0), part, o)
    for part in range(3):
        for o in near:
            send(
                ("a1o", part, o), block(xg, part, 0, 0, 0), block(xg, part, 0, 4 - o, 0), part + 1, o
            )
    local = []
    for n, (src, dst) in enumerate(
        (
            (eg_ref, wg.at[mine]), (eu_ref, wu.at[mine]), (ed_ref, wd.at[mine]),
            (sg_ref, sgv), (su_ref, suv), (sd_ref, sdv),
        )
    ):
        copy = pltpu.make_async_copy(src, dst, w_local.at[n])
        copy.start()
        local.append(copy)

    for n in range(3):
        swap(n, mine).start()
    for part in range(3):
        for o in near:
            arrive("a0", part, o)
        for o in near:
            send(
                ("a1", part, o), block(xg, part, REST, 0, 0), block(xg, part, REST, 4 - o, 0), part + 1, o
            )
    for part in range(3):
        for o in near:
            send(
                ("a2l", part, o), block(xg, part, ALL, 0, 0), block(xg, part, ALL, 0, 4 - o), part + 2, o
            )
    for o in near:
        arrive("a1o", 0, o)
        arrive("a1", 0, o)
    for k in ORDER:
        for o in near:
            send(("a2", 0, k, o), block(xg, 0, k, REST, 0), block(xg, 0, k, REST, 4 - o), 2, o)
    for o in near:
        arrive("a1o", 1, o)
        arrive("a1", 1, o)
    for o in near:
        send(("a2", 1, o), block(xg, 1, ALL, REST, 0), block(xg, 1, ALL, REST, 4 - o), 0, o)
    for q in near:
        arrive("a1o", 2, 4 - q)
        arrive("a1", 2, 4 - q)
        for o in near:
            send(("a2", 2, q, o), block(xg, 2, ALL, q, 0), block(xg, 2, ALL, q, 4 - o), 1, o)

    for copy in local:
        copy.wait()
    own = xg[0, 0, 0, :, 0:D]
    part_g = jnp.dot(own, sgv[...], preferred_element_type=F32)
    part_u = jnp.dot(own, suv[...], preferred_element_type=F32)
    hidden = (part_g / (1.0 + jnp.exp(-part_g)) * part_u).astype(BF)
    total[...] = jnp.dot(hidden, sdv[...], preferred_element_type=F32)

    for n in range(3):
        swap(n, theirs).wait_recv()

    r1, s1 = (r1a, r1b, r1c), (s1a, s1b, s1c)
    r2, s2 = (r2a, r2b, r2c), (s2a, s2b, s2c)
    r3 = (r3a, r3b, r3c)

    def out_block(part, i, j, k):
        return block(yb, part, i, j, k, WIDTH[part])

    wide_lane = lax.broadcasted_iota(jnp.int32, (256, 128), 1)
    for k in ORDER:
        if k == 0:
            for o in near:
                arrive("a2l", 0, o)
                arrive("a2l", 2, o)
        else:
            arrive("a2l", 1, 4 - k)
            arrive("a2", 1, 4 - k)
        for o in near:
            arrive("a2", 0, k, o)
            if k != 0:
                arrive("a2", 2, k, o)
        info = xg[k, :, :, :, D:WIDE].reshape(256, 128).astype(F32)
        weights = pltpu.roll(info, 120, 1) + pltpu.roll(info, 112, 1)
        x = xg[k, :, :, :, 0:D].reshape(256, D)
        for e in range(4):
            name = (4 * chip + e).astype(F32)
            hit = jnp.where((info == name) & (wide_lane < 8), weights, 0.0)
            w = jnp.sum(hit, axis=1, keepdims=True)
            g = jnp.dot(x, wg[e], preferred_element_type=F32)
            u = jnp.dot(x, wu[e], preferred_element_type=F32)
            hs[:, 256 * e : 256 * e + 256] = (g / (1.0 + jnp.exp(-g)) * u * w).astype(BF)
        y = jnp.dot(hs[...], wd[...].reshape(D, D), preferred_element_type=F32)
        yb[k] = y.astype(BF).reshape(4, 4, 16, D)
        for o in near:
            send(("r1", 0, k, o), out_block(0, k, REST, o), r1a.at[o - 1, k, REST], 2, o)
            if k != 0:
                send(("r1", 2, k, o), out_block(2, ALL, k, o), r1c.at[o - 1, k], 1, o)
        if k != 0:
            send(("r1", 1, k), out_block(1, ALL, REST, k), r1b.at[k - 1, :, REST], 0, k)
    for o in near:
        send(("r1l", 0, o), out_block(0, ALL, 0, o), r1a.at[o - 1, :, 0], 2, o)
        send(("r1l", 1, o), out_block(1, ALL, 0, o), r1b.at[o - 1, :, 0], 0, o)
        send(("r1l", 2, o), out_block(2, ALL, 0, o), r1c.at[o - 1, 0], 1, o)

    for k in (1, 3, 2):
        for o in near:
            arrive("r1", 2, k, o)
        acc = yb[k, 0, :, :, 2 * CUT : D].astype(F32)
        for o in (1, 2, 3):
            acc = acc + r1c[o - 1, k].astype(F32)
        s1c[k] = acc.astype(BF)
        send(("r2", 2, k), s1c.at[k, REST], r2c.at[k - 1, REST], 0, k)
    for o in near:
        arrive("r1", 1, o)
    acc = yb[0, :, 1:4, :, CUT : 2 * CUT].astype(F32)
    for o in (1, 2, 3):
        acc = acc + r1b[o - 1, :, 1:4].astype(F32)
    s1b[:, 1:4] = acc.astype(BF)
    for o in near:
        send(("r2", 1, o), s1b.at[REST, o], r2b.at[o - 1, REST], 2, o)
    for o in near:
        for k in ORDER:
            arrive("r1", 0, k, o)
    acc = yb[:, 1:4, 0, :, 0:CUT].astype(F32)
    for o in (1, 2, 3):
        acc = acc + r1a[o - 1, :, 1:4].astype(F32)
    s1a[:, 1:4] = acc.astype(BF)
    for o in near:
        send(("r2", 0, o), s1a.at[REST, o], r2a.at[o - 1, REST], 1, o)
    for o in near:
        send(("r2l", 2, o), s1c.at[o, 0], r2c.at[o - 1, 0], 0, o)
        send(("r2l", 1, o), s1b.at[0, o], r2b.at[o - 1, 0], 2, o)
        send(("r2l", 0, o), s1a.at[0, o], r2a.at[o - 1, 0], 1, o)

    drain("a0", "a1o", "a1", "a2l", "a2")
    for n in range(3):
        swap(n, mine).wait_send()

    for part in (2, 1, 0):
        for o in near:
            arrive("r1l", part, o)
        if part == 0:
            acc = yb[:, 0, 0, :, 0:CUT].astype(F32)
        elif part == 1:
            acc = yb[0, :, 0, :, CUT : 2 * CUT].astype(F32)
        else:
            acc = yb[0, 0, :, :, 2 * CUT : D].astype(F32)
        for o in (1, 2, 3):
            line = r1c[o - 1, 0] if part == 2 else r1[part][o - 1, :, 0]
            acc = acc + line.astype(F32)
        total[:, CUT * part : CUT * part + WIDTH[part]] += acc[0]
        for o in near:
            arrive("r2", part, o)
        acc = acc[1:4]
        for o in (1, 2, 3):
            acc = acc + r2[part][o - 1, 1:4].astype(F32)
        s2[part][1:4] = acc.astype(BF)
        for o in near:
            send(("r3", part, o), s2[part].at[o], r3[part].at[o - 1], part, o)
    drain("r1", "r1l", "r2", "r2l")
    for part in (2, 1, 0):
        for o in near:
            arrive("r2l", part, o)
        acc = r2[part][0, 0].astype(F32)
        for o in (2, 3):
            acc = acc + r2[part][o - 1, 0].astype(F32)
        for o in near:
            arrive("r3", part, o)
        for o in (1, 2, 3):
            acc = acc + r3[part][o - 1].astype(F32)
        total[:, CUT * part : CUT * part + WIDTH[part]] += acc

    summed = total[...]
    mean = jnp.mean(summed * summed, axis=-1, keepdims=True)
    mixed = jnp.where(live, summed * lax.rsqrt(mean + EPS) * og_ref[...], 0.0)
    mixed = mixed.astype(BF)
    for s in range(4):
        out_ref[s] = mixed[4 * s : 4 * s + 4, :]
    drain("r3")


def per_device(
    tokens, lengths, routes, gates, norm_gain,
    expert_gate, expert_up, expert_down, shared_gate, shared_up, shared_down, out_gain,
):
    vmem = pl.BlockSpec(memory_space=pltpu.VMEM)
    hbm = pl.BlockSpec(memory_space=pltpu.HBM)
    dma = pltpu.SemaphoreType.DMA
    buffers = [pltpu.VMEM((4, 4, 4, 16, WIDE), BF), pltpu.VMEM((4, 4, 4, 16, D), BF)]
    buffers += [pltpu.VMEM((3, 4, 4, 16, w), BF) for w in WIDTH]
    buffers += [pltpu.VMEM((4, 4, 16, w), BF) for w in WIDTH]
    buffers += [pltpu.VMEM((3, 4, 16, w), BF) for w in WIDTH]
    buffers += [pltpu.VMEM((4, 16, w), BF) for w in WIDTH]
    buffers += [pltpu.VMEM((3, 16, w), BF) for w in WIDTH]
    buffers += [
        pltpu.VMEM((4, D, 256), BF), pltpu.VMEM((4, D, 256), BF), pltpu.VMEM((4, 256, D), BF),
        pltpu.VMEM((D, 256), BF), pltpu.VMEM((D, 256), BF), pltpu.VMEM((256, D), BF),
        pltpu.VMEM((16, D), F32), pltpu.VMEM((16, 128), F32), pltpu.VMEM((16, 128), F32),
        pltpu.VMEM((256, D), BF), pltpu.VMEM((16, D), F32),
        pltpu.SMEM((4,), jnp.int32), pltpu.VMEM((4, 4, D), BF),
        pltpu.VMEM((4, 4, 8), jnp.int32), pltpu.VMEM((4, 4, 8), F32),
        pltpu.VMEM((1, D), F32), pltpu.VMEM((1, D), F32),
    ]
    return pl.pallas_call(
        kernel,
        out_shape=jax.ShapeDtypeStruct(tokens.shape, BF),
        in_specs=[hbm] * 12,
        out_specs=vmem,
        scratch_shapes=buffers
        + [dma((120,)), dma((120,)), dma((3,)), dma((3,)), dma((6,)), dma((6,))],
        compiler_params=pltpu.CompilerParams(
            collective_id=0, has_side_effects=True, vmem_limit_bytes=67043328
        ),
    )(
        lengths, tokens, routes, gates, norm_gain.reshape(1, D), out_gain.reshape(1, D),
        expert_gate, expert_up, expert_down, shared_gate, shared_up, shared_down,
    )


def solution(mesh):
    placed = (
        P("ep", None, None), P("ep"), P("ep", None, None), P("ep", None, None), P(),
        P("ep", None, None), P("ep", None, None), P("ep", None, None), P(), P(), P(), P(),
    )
    return jax.shard_map(
        per_device, mesh=mesh, in_specs=placed, out_specs=P("ep", None, None), check_vma=False
    )
```

```python
import jax
import jax.numpy as jnp
from jax import lax
from jax.experimental import pallas as pl
from jax.experimental.pallas import tpu as pltpu
from jax.sharding import PartitionSpec as P

MESH = pl.DeviceIdType.MESH
EPS = 1e-06
BF = jnp.bfloat16
F32 = jnp.float32
D = 1024
WIDE = 1152
CUT = 384
WIDTH = (384, 384, 256)
ORDER = (0, 1, 3, 2)
REST = slice(1, 4)
ALL = slice(None)


def kernel(
    lengths_hbm, tokens_hbm, routes_hbm, gates_hbm, ng_hbm, og_hbm,
    eg_ref, eu_ref, ed_ref, sg_ref, su_ref, sd_ref,
    out_ref,
    xg, yb, r1a, r1b, r1c, s1a, s1b, s1c, r2a, r2b, r2c, s2a, s2b, s2c, r3a, r3b, r3c,
    wg, wu, wd, sgv, suv, sdv, rows, meta_a, meta_b, hs, total,
    lengths_ref, tokens_ref, routes_ref, gates_ref, ng_ref, og_ref,
    send_sem, recv_sem, w_send, w_recv, w_local, small,
):
    me = lax.axis_index("ep")
    core = lax.rem(me, 2)
    chip = me // 2
    c = (chip // 16, lax.rem(chip // 4, 4), lax.rem(chip, 4))
    stride = (32, 8, 2)
    partner = me + 1 - 2 * core

    peers = [
        [me + (lax.rem(c[dim] + o, 4) - c[dim]) * stride[dim] for o in range(4)]
        for dim in range(3)
    ]

    barrier = pltpu.get_barrier_semaphore()
    for o in (2, 3, 1):
        for dim in range(3):
            pl.semaphore_signal(
                barrier, inc=1, device_id=(peers[dim][o],), device_id_type=MESH
            )
    pl.semaphore_signal(barrier, inc=1, device_id=(partner,), device_id_type=MESH)

    early = []
    for n, (src, dst) in enumerate(
        (
            (tokens_hbm, tokens_ref), (ng_hbm, ng_ref), (routes_hbm, routes_ref),
            (gates_hbm, gates_ref), (lengths_hbm, lengths_ref), (og_hbm, og_ref),
        )
    ):
        copy = pltpu.make_async_copy(src, dst, small.at[n])
        copy.start()
        early.append(copy)
    mine = pl.ds(2 * core, 2)
    row = lax.broadcasted_iota(jnp.int32, (16, 1), 0)
    early[0].wait()
    early[1].wait()
    for s in range(4):
        rows[4 * s : 4 * s + 4, :] = tokens_ref[s].astype(F32)
    values = rows[...]
    mean = jnp.mean(values * values, axis=-1, keepdims=True)
    normed = (values * lax.rsqrt(mean + EPS) * ng_ref[...]).astype(BF)
    xg[0, 0, 0, :, 0:D] = normed

    for copy in early[2:]:
        copy.wait()
    limit = jnp.zeros((16, 1), jnp.int32)
    for s in range(4):
        limit = jnp.where(row // 4 == s, lengths_ref[s], limit)
        meta_a[4 * s : 4 * s + 4, 0:8] = routes_ref[s].astype(F32)
        meta_b[4 * s : 4 * s + 4, 0:8] = gates_ref[s]
    live = lax.rem(row, 4) < limit
    pl.semaphore_wait(barrier, 10)

    def swap(n, dst_slot):
        src, dst = ((eg_ref, wg), (eu_ref, wu), (ed_ref, wd))[n]
        return pltpu.make_async_remote_copy(
            src_ref=src, dst_ref=dst.at[dst_slot], send_sem=w_send.at[n],
            recv_sem=w_recv.at[n], device_id=(partner,), device_id_type=MESH,
        )

    theirs = pl.ds(2 - 2 * core, 2)

    copies = {}

    def block(ref, part, i, j, k, width=CUT):
        index = [0, 0, 0]
        index[part], index[(part + 1) % 3], index[(part + 2) % 3] = i, j, k
        return ref.at[index[0], index[1], index[2], :, pl.ds(CUT * part, width)]

    def send(key, src, dst, dim, o):
        n = len(copies)
        copies[key] = pltpu.make_async_remote_copy(
            src_ref=src, dst_ref=dst, send_sem=send_sem.at[n], recv_sem=recv_sem.at[n],
            device_id=(peers[dim % 3][o],), device_id_type=MESH,
        )
        copies[key].start()

    def arrive(*key):
        copies[key].wait_recv()

    def drain(*kinds):
        for key in copies:
            if key[0] in kinds:
                copies[key].wait_send()

    near = (1, 3, 2)
    for part in range(3):
        if part == 2:
            lane = lax.broadcasted_iota(jnp.int32, (16, 128), 1)
            ids = jnp.where(live, meta_a[...], -1.0)
            gate = meta_b[...]
            high = gate.astype(BF).astype(F32)
            low = gate - high
            packed = jnp.where(
                lane < 8,
                ids,
                jnp.where(
                    lane < 16,
                    pltpu.roll(high, 8, 1),
                    jnp.where(lane < 24, pltpu.roll(low, 16, 1), 0.0),
                ),
            )
            xg[0, 0, 0, :, D:WIDE] = packed.astype(BF)
        for o in near:
            send(("a0", part, o), block(xg, part, 0, 0, 0), block(xg, part, 4 - o, 0, 0), part, o)
    for part in range(3):
        for o in near:
            send(
                ("a1o", part, o), block(xg, part, 0, 0, 0), block(xg, part, 0, 4 - o, 0), part + 1, o
            )
    local = []
    for n, (src, dst) in enumerate(
        (
            (eg_ref, wg.at[mine]), (eu_ref, wu.at[mine]), (ed_ref, wd.at[mine]),
            (sg_ref, sgv), (su_ref, suv), (sd_ref, sdv),
        )
    ):
        copy = pltpu.make_async_copy(src, dst, w_local.at[n])
        copy.start()
        local.append(copy)

    for n in range(3):
        swap(n, mine).start()
    for part in range(3):
        for o in near:
            arrive("a0", part, o)
        for o in near:
            send(
                ("a1", part, o), block(xg, part, REST, 0, 0), block(xg, part, REST, 4 - o, 0), part + 1, o
            )
    for part in range(3):
        for o in near:
            send(
                ("a2l", part, o), block(xg, part, ALL, 0, 0), block(xg, part, ALL, 0, 4 - o), part + 2, o
            )
    for o in near:
        arrive("a1o", 0, o)
        arrive("a1", 0, o)
    for k in ORDER:
        for o in near:
            send(("a2", 0, k, o), block(xg, 0, k, REST, 0), block(xg, 0, k, REST, 4 - o), 2, o)
    for o in near:
        arrive("a1o", 1, o)
        arrive("a1", 1, o)
    for o in near:
        send(("a2", 1, o), block(xg, 1, ALL, REST, 0), block(xg, 1, ALL, REST, 4 - o), 0, o)
    for q in near:
        arrive("a1o", 2, 4 - q)
        arrive("a1", 2, 4 - q)
        for o in near:
            send(("a2", 2, q, o), block(xg, 2, ALL, q, 0), block(xg, 2, ALL, q, 4 - o), 1, o)

    for copy in local:
        copy.wait()

    for n in range(3):
        swap(n, theirs).wait_recv()

    r1, s1 = (r1a, r1b, r1c), (s1a, s1b, s1c)
    r2, s2 = (r2a, r2b, r2c), (s2a, s2b, s2c)
    r3 = (r3a, r3b, r3c)

    def out_block(part, i, j, k):
        return block(yb, part, i, j, k, WIDTH[part])

    wide_lane = lax.broadcasted_iota(jnp.int32, (256, 128), 1)
    for k in ORDER:
        if k == 0:
            for o in near:
                arrive("a2l", 0, o)
                arrive("a2l", 2, o)
        else:
            arrive("a2l", 1, 4 - k)
            arrive("a2", 1, 4 - k)
        for o in near:
            arrive("a2", 0, k, o)
            if k != 0:
                arrive("a2", 2, k, o)
        info = xg[k, :, :, :, D:WIDE].reshape(256, 128).astype(F32)
        weights = pltpu.roll(info, 120, 1) + pltpu.roll(info, 112, 1)
        x = xg[k, :, :, :, 0:D].reshape(256, D)
        for e in range(4):
            name = (4 * chip + e).astype(F32)
            hit = jnp.where((info == name) & (wide_lane < 8), weights, 0.0)
            w = jnp.sum(hit, axis=1, keepdims=True)
            g = jnp.dot(x, wg[e], preferred_element_type=F32)
            u = jnp.dot(x, wu[e], preferred_element_type=F32)
            hs[:, 256 * e : 256 * e + 256] = (g / (1.0 + jnp.exp(-g)) * u * w).astype(BF)
        y = jnp.dot(hs[...], wd[...].reshape(D, D), preferred_element_type=F32)
        yb[k] = y.astype(BF).reshape(4, 4, 16, D)
        for o in near:
            send(("r1", 0, k, o), out_block(0, k, REST, o), r1a.at[o - 1, k, REST], 2, o)
            if k != 0:
                send(("r1", 2, k, o), out_block(2, ALL, k, o), r1c.at[o - 1, k], 1, o)
        if k != 0:
            send(("r1", 1, k), out_block(1, ALL, REST, k), r1b.at[k - 1, :, REST], 0, k)
            send(("r1l", 1, k), out_block(1, ALL, 0, k), r1b.at[k - 1, :, 0], 0, k)
        if k == 3:
            for o in near:
                send(("r1l", 2, o), out_block(2, ALL, 0, o), r1c.at[o - 1, 0], 1, o)
    for o in near:
        send(("r1l", 0, o), out_block(0, ALL, 0, o), r1a.at[o - 1, :, 0], 2, o)

    for k in (1, 3, 2):
        for o in near:
            arrive("r1", 2, k, o)
        acc = yb[k, 0, :, :, 2 * CUT : D].astype(F32)
        for o in (1, 2, 3):
            acc = acc + r1c[o - 1, k].astype(F32)
        s1c[k] = acc.astype(BF)
        send(("r2", 2, k), s1c.at[k, REST], r2c.at[k - 1, REST], 0, k)
    for o in near:
        arrive("r1", 1, o)
    acc = yb[0, :, 1:4, :, CUT : 2 * CUT].astype(F32)
    for o in (1, 2, 3):
        acc = acc + r1b[o - 1, :, 1:4].astype(F32)
    s1b[:, 1:4] = acc.astype(BF)
    for o in near:
        send(("r2", 1, o), s1b.at[REST, o], r2b.at[o - 1, REST], 2, o)
    for o in near:
        for k in ORDER:
            arrive("r1", 0, k, o)
    acc = yb[:, 1:4, 0, :, 0:CUT].astype(F32)
    for o in (1, 2, 3):
        acc = acc + r1a[o - 1, :, 1:4].astype(F32)
    s1a[:, 1:4] = acc.astype(BF)
    for o in near:
        send(("r2", 0, o), s1a.at[REST, o], r2a.at[o - 1, REST], 1, o)
    for o in near:
        send(("r2l", 2, o), s1c.at[o, 0], r2c.at[o - 1, 0], 0, o)
        send(("r2l", 1, o), s1b.at[0, o], r2b.at[o - 1, 0], 2, o)
        send(("r2l", 0, o), s1a.at[0, o], r2a.at[o - 1, 0], 1, o)

    own = xg[0, 0, 0, :, 0:D]
    part_g = jnp.dot(own, sgv[...], preferred_element_type=F32)
    part_u = jnp.dot(own, suv[...], preferred_element_type=F32)
    hidden = (part_g / (1.0 + jnp.exp(-part_g)) * part_u).astype(BF)
    total[...] = jnp.dot(hidden, sdv[...], preferred_element_type=F32)
    drain("a0", "a1o", "a1", "a2l", "a2")
    for n in range(3):
        swap(n, mine).wait_send()

    for part in (2, 1, 0):
        for o in near:
            arrive("r1l", part, o)
        if part == 0:
            acc = yb[:, 0, 0, :, 0:CUT].astype(F32)
        elif part == 1:
            acc = yb[0, :, 0, :, CUT : 2 * CUT].astype(F32)
        else:
            acc = yb[0, 0, :, :, 2 * CUT : D].astype(F32)
        for o in (1, 2, 3):
            line = r1c[o - 1, 0] if part == 2 else r1[part][o - 1, :, 0]
            acc = acc + line.astype(F32)
        total[:, CUT * part : CUT * part + WIDTH[part]] += acc[0]
        for o in near:
            arrive("r2", part, o)
        acc = acc[1:4]
        for o in (1, 2, 3):
            acc = acc + r2[part][o - 1, 1:4].astype(F32)
        s2[part][1:4] = acc.astype(BF)
        for o in near:
            send(("r3", part, o), s2[part].at[o], r3[part].at[o - 1], part, o)
    drain("r1", "r1l", "r2", "r2l")
    for part in (2, 1, 0):
        for o in near:
            arrive("r2l", part, o)
        acc = r2[part][0, 0].astype(F32)
        for o in (2, 3):
            acc = acc + r2[part][o - 1, 0].astype(F32)
        for o in near:
            arrive("r3", part, o)
        for o in (1, 2, 3):
            acc = acc + r3[part][o - 1].astype(F32)
        total[:, CUT * part : CUT * part + WIDTH[part]] += acc

    summed = total[...]
    mean = jnp.mean(summed * summed, axis=-1, keepdims=True)
    mixed = jnp.where(live, summed * lax.rsqrt(mean + EPS) * og_ref[...], 0.0)
    mixed = mixed.astype(BF)
    for s in range(4):
        out_ref[s] = mixed[4 * s : 4 * s + 4, :]
    drain("r3")


def per_device(
    tokens, lengths, routes, gates, norm_gain,
    expert_gate, expert_up, expert_down, shared_gate, shared_up, shared_down, out_gain,
):
    vmem = pl.BlockSpec(memory_space=pltpu.VMEM)
    hbm = pl.BlockSpec(memory_space=pltpu.HBM)
    dma = pltpu.SemaphoreType.DMA
    buffers = [pltpu.VMEM((4, 4, 4, 16, WIDE), BF), pltpu.VMEM((4, 4, 4, 16, D), BF)]
    buffers += [pltpu.VMEM((3, 4, 4, 16, w), BF) for w in WIDTH]
    buffers += [pltpu.VMEM((4, 4, 16, w), BF) for w in WIDTH]
    buffers += [pltpu.VMEM((3, 4, 16, w), BF) for w in WIDTH]
    buffers += [pltpu.VMEM((4, 16, w), BF) for w in WIDTH]
    buffers += [pltpu.VMEM((3, 16, w), BF) for w in WIDTH]
    buffers += [
        pltpu.VMEM((4, D, 256), BF), pltpu.VMEM((4, D, 256), BF), pltpu.VMEM((4, 256, D), BF),
        pltpu.VMEM((D, 256), BF), pltpu.VMEM((D, 256), BF), pltpu.VMEM((256, D), BF),
        pltpu.VMEM((16, D), F32), pltpu.VMEM((16, 128), F32), pltpu.VMEM((16, 128), F32),
        pltpu.VMEM((256, D), BF), pltpu.VMEM((16, D), F32),
        pltpu.SMEM((4,), jnp.int32), pltpu.VMEM((4, 4, D), BF),
        pltpu.VMEM((4, 4, 8), jnp.int32), pltpu.VMEM((4, 4, 8), F32),
        pltpu.VMEM((1, D), F32), pltpu.VMEM((1, D), F32),
    ]
    return pl.pallas_call(
        kernel,
        out_shape=jax.ShapeDtypeStruct(tokens.shape, BF),
        in_specs=[hbm] * 12,
        out_specs=vmem,
        scratch_shapes=buffers
        + [dma((120,)), dma((120,)), dma((3,)), dma((3,)), dma((6,)), dma((6,))],
        compiler_params=pltpu.CompilerParams(
            collective_id=0, has_side_effects=True, vmem_limit_bytes=67043328
        ),
    )(
        lengths, tokens, routes, gates, norm_gain.reshape(1, D), out_gain.reshape(1, D),
        expert_gate, expert_up, expert_down, shared_gate, shared_up, shared_down,
    )


def solution(mesh):
    placed = (
        P("ep", None, None), P("ep"), P("ep", None, None), P("ep", None, None), P(),
        P("ep", None, None), P("ep", None, None), P("ep", None, None), P(), P(), P(), P(),
    )
    return jax.shard_map(
        per_device, mesh=mesh, in_specs=placed, out_specs=P("ep", None, None), check_vma=False
    )
```

```python
import jax
import jax.numpy as jnp
from jax import lax
from jax.experimental import pallas as pl
from jax.experimental.pallas import tpu as pltpu
from jax.sharding import PartitionSpec as P

MESH = pl.DeviceIdType.MESH
EPS = 1e-06
BF = jnp.bfloat16
F32 = jnp.float32
D = 1024
WIDE = 1152
CUT = 384
WIDTH = (384, 384, 256)
ORDER = (0, 1, 3, 2)
REST = slice(1, 4)
ALL = slice(None)


def kernel(
    lengths_hbm, tokens_hbm, routes_hbm, gates_hbm, ng_hbm, og_hbm,
    eg_ref, eu_ref, ed_ref, sg_ref, su_ref, sd_ref,
    out_ref,
    xg, yb, r1a, r1b, r1c, s1a, s1b, s1c, r2a, r2b, r2c, s2a, s2b, s2c, r3a, r3b, r3c,
    wg, wu, wd, sgv, suv, sdv, rows, meta_a, meta_b, hs, total,
    lengths_ref, tokens_ref, routes_ref, gates_ref, ng_ref, og_ref,
    send_sem, recv_sem, w_send, w_recv, w_local, small,
):
    me = lax.axis_index("ep")
    core = lax.rem(me, 2)
    chip = me // 2
    c = (chip // 16, lax.rem(chip // 4, 4), lax.rem(chip, 4))
    stride = (32, 8, 2)
    partner = me + 1 - 2 * core

    peers = [
        [me + (lax.rem(c[dim] + o, 4) - c[dim]) * stride[dim] for o in range(4)]
        for dim in range(3)
    ]

    early = []
    for n, (src, dst) in enumerate(
        (
            (tokens_hbm, tokens_ref), (ng_hbm, ng_ref), (routes_hbm, routes_ref),
            (gates_hbm, gates_ref), (lengths_hbm, lengths_ref), (og_hbm, og_ref),
        )
    ):
        copy = pltpu.make_async_copy(src, dst, small.at[n])
        copy.start()
        early.append(copy)

    barrier = pltpu.get_barrier_semaphore()
    for o in (2, 3, 1):
        for dim in range(3):
            pl.semaphore_signal(
                barrier, inc=1, device_id=(peers[dim][o],), device_id_type=MESH
            )
    pl.semaphore_signal(barrier, inc=1, device_id=(partner,), device_id_type=MESH)
    mine = pl.ds(2 * core, 2)
    row = lax.broadcasted_iota(jnp.int32, (16, 1), 0)
    early[0].wait()
    early[1].wait()
    for s in range(4):
        rows[4 * s : 4 * s + 4, :] = tokens_ref[s].astype(F32)
    values = rows[...]
    mean = jnp.mean(values * values, axis=-1, keepdims=True)
    normed = (values * lax.rsqrt(mean + EPS) * ng_ref[...]).astype(BF)
    xg[0, 0, 0, :, 0:D] = normed

    for copy in early[2:]:
        copy.wait()
    limit = jnp.zeros((16, 1), jnp.int32)
    for s in range(4):
        limit = jnp.where(row // 4 == s, lengths_ref[s], limit)
        meta_a[4 * s : 4 * s + 4, 0:8] = routes_ref[s].astype(F32)
        meta_b[4 * s : 4 * s + 4, 0:8] = gates_ref[s]
    live = lax.rem(row, 4) < limit
    pl.semaphore_wait(barrier, 10)

    def swap(n, dst_slot):
        src, dst = ((eg_ref, wg), (eu_ref, wu), (ed_ref, wd))[n]
        return pltpu.make_async_remote_copy(
            src_ref=src, dst_ref=dst.at[dst_slot], send_sem=w_send.at[n],
            recv_sem=w_recv.at[n], device_id=(partner,), device_id_type=MESH,
        )

    theirs = pl.ds(2 - 2 * core, 2)

    copies = {}

    def block(ref, part, i, j, k, width=CUT):
        index = [0, 0, 0]
        index[part], index[(part + 1) % 3], index[(part + 2) % 3] = i, j, k
        return ref.at[index[0], index[1], index[2], :, pl.ds(CUT * part, width)]

    def send(key, src, dst, dim, o):
        n = len(copies)
        copies[key] = pltpu.make_async_remote_copy(
            src_ref=src, dst_ref=dst, send_sem=send_sem.at[n], recv_sem=recv_sem.at[n],
            device_id=(peers[dim % 3][o],), device_id_type=MESH,
        )
        copies[key].start()

    def arrive(*key):
        copies[key].wait_recv()

    def drain(*kinds):
        for key in copies:
            if key[0] in kinds:
                copies[key].wait_send()

    near = (1, 3, 2)
    for part in range(3):
        if part == 2:
            lane = lax.broadcasted_iota(jnp.int32, (16, 128), 1)
            ids = jnp.where(live, meta_a[...], -1.0)
            gate = meta_b[...]
            high = gate.astype(BF).astype(F32)
            low = gate - high
            packed = jnp.where(
                lane < 8,
                ids,
                jnp.where(
                    lane < 16,
                    pltpu.roll(high, 8, 1),
                    jnp.where(lane < 24, pltpu.roll(low, 16, 1), 0.0),
                ),
            )
            xg[0, 0, 0, :, D:WIDE] = packed.astype(BF)
        for o in near:
            send(("a0", part, o), block(xg, part, 0, 0, 0), block(xg, part, 4 - o, 0, 0), part, o)
    for part in range(3):
        for o in near:
            send(
                ("a1o", part, o), block(xg, part, 0, 0, 0), block(xg, part, 0, 4 - o, 0), part + 1, o
            )
    local = []
    for n, (src, dst) in enumerate(
        (
            (eg_ref, wg.at[mine]), (eu_ref, wu.at[mine]), (ed_ref, wd.at[mine]),
            (sg_ref, sgv), (su_ref, suv), (sd_ref, sdv),
        )
    ):
        copy = pltpu.make_async_copy(src, dst, w_local.at[n])
        copy.start()
        local.append(copy)

    for n in range(3):
        swap(n, mine).start()
    for part in range(3):
        for o in near:
            arrive("a0", part, o)
        for o in near:
            send(
                ("a1", part, o), block(xg, part, REST, 0, 0), block(xg, part, REST, 4 - o, 0), part + 1, o
            )
    for part in range(3):
        for o in near:
            send(
                ("a2l", part, o), block(xg, part, ALL, 0, 0), block(xg, part, ALL, 0, 4 - o), part + 2, o
            )
    for o in near:
        arrive("a1o", 0, o)
        arrive("a1", 0, o)
    for k in ORDER:
        for o in near:
            send(("a2", 0, k, o), block(xg, 0, k, REST, 0), block(xg, 0, k, REST, 4 - o), 2, o)
    for o in near:
        arrive("a1o", 1, o)
        arrive("a1", 1, o)
    for o in near:
        send(("a2", 1, o), block(xg, 1, ALL, REST, 0), block(xg, 1, ALL, REST, 4 - o), 0, o)
    for q in near:
        arrive("a1o", 2, 4 - q)
        arrive("a1", 2, 4 - q)
        for o in near:
            send(("a2", 2, q, o), block(xg, 2, ALL, q, 0), block(xg, 2, ALL, q, 4 - o), 1, o)

    for copy in local:
        copy.wait()

    for n in range(3):
        swap(n, theirs).wait_recv()

    r1, s1 = (r1a, r1b, r1c), (s1a, s1b, s1c)
    r2, s2 = (r2a, r2b, r2c), (s2a, s2b, s2c)
    r3 = (r3a, r3b, r3c)

    def out_block(part, i, j, k):
        return block(yb, part, i, j, k, WIDTH[part])

    wide_lane = lax.broadcasted_iota(jnp.int32, (256, 128), 1)
    for k in ORDER:
        if k == 0:
            for o in near:
                arrive("a2l", 0, o)
                arrive("a2l", 2, o)
        else:
            arrive("a2l", 1, 4 - k)
            arrive("a2", 1, 4 - k)
        for o in near:
            arrive("a2", 0, k, o)
            if k != 0:
                arrive("a2", 2, k, o)
        info = xg[k, :, :, :, D:WIDE].reshape(256, 128).astype(F32)
        weights = pltpu.roll(info, 120, 1) + pltpu.roll(info, 112, 1)
        x = xg[k, :, :, :, 0:D].reshape(256, D)
        for e in range(4):
            name = (4 * chip + e).astype(F32)
            hit = jnp.where((info == name) & (wide_lane < 8), weights, 0.0)
            w = jnp.sum(hit, axis=1, keepdims=True)
            g = jnp.dot(x, wg[e], preferred_element_type=F32)
            u = jnp.dot(x, wu[e], preferred_element_type=F32)
            hs[:, 256 * e : 256 * e + 256] = (g / (1.0 + jnp.exp(-g)) * u * w).astype(BF)
        y = jnp.dot(hs[...], wd[...].reshape(D, D), preferred_element_type=F32)
        yb[k] = y.astype(BF).reshape(4, 4, 16, D)
        for o in near:
            send(("r1", 0, k, o), out_block(0, k, REST, o), r1a.at[o - 1, k, REST], 2, o)
            if k != 0:
                send(("r1", 2, k, o), out_block(2, ALL, k, o), r1c.at[o - 1, k], 1, o)
        if k != 0:
            send(("r1", 1, k), out_block(1, ALL, REST, k), r1b.at[k - 1, :, REST], 0, k)
            send(("r1l", 1, k), out_block(1, ALL, 0, k), r1b.at[k - 1, :, 0], 0, k)
        if k == 3:
            for o in near:
                send(("r1l", 2, o), out_block(2, ALL, 0, o), r1c.at[o - 1, 0], 1, o)
    for o in near:
        send(("r1l", 0, o), out_block(0, ALL, 0, o), r1a.at[o - 1, :, 0], 2, o)

    for k in (1, 3, 2):
        for o in near:
            arrive("r1", 2, k, o)
        acc = yb[k, 0, :, :, 2 * CUT : D].astype(F32)
        for o in (1, 2, 3):
            acc = acc + r1c[o - 1, k].astype(F32)
        s1c[k] = acc.astype(BF)
        send(("r2", 2, k), s1c.at[k, REST], r2c.at[k - 1, REST], 0, k)
    for o in near:
        arrive("r1", 1, o)
    acc = yb[0, :, 1:4, :, CUT : 2 * CUT].astype(F32)
    for o in (1, 2, 3):
        acc = acc + r1b[o - 1, :, 1:4].astype(F32)
    s1b[:, 1:4] = acc.astype(BF)
    for o in near:
        send(("r2", 1, o), s1b.at[REST, o], r2b.at[o - 1, REST], 2, o)
    for o in near:
        for k in ORDER:
            arrive("r1", 0, k, o)
    acc = yb[:, 1:4, 0, :, 0:CUT].astype(F32)
    for o in (1, 2, 3):
        acc = acc + r1a[o - 1, :, 1:4].astype(F32)
    s1a[:, 1:4] = acc.astype(BF)
    for o in near:
        send(("r2", 0, o), s1a.at[REST, o], r2a.at[o - 1, REST], 1, o)
    for o in near:
        send(("r2l", 2, o), s1c.at[o, 0], r2c.at[o - 1, 0], 0, o)
        send(("r2l", 1, o), s1b.at[0, o], r2b.at[o - 1, 0], 2, o)
        send(("r2l", 0, o), s1a.at[0, o], r2a.at[o - 1, 0], 1, o)

    own = xg[0, 0, 0, :, 0:D]
    part_g = jnp.dot(own, sgv[...], preferred_element_type=F32)
    part_u = jnp.dot(own, suv[...], preferred_element_type=F32)
    hidden = (part_g / (1.0 + jnp.exp(-part_g)) * part_u).astype(BF)
    total[...] = jnp.dot(hidden, sdv[...], preferred_element_type=F32)
    drain("a0", "a1o", "a1", "a2l", "a2")
    for n in range(3):
        swap(n, mine).wait_send()

    for part in (2, 1, 0):
        for o in near:
            arrive("r1l", part, o)
        if part == 0:
            acc = yb[:, 0, 0, :, 0:CUT].astype(F32)
        elif part == 1:
            acc = yb[0, :, 0, :, CUT : 2 * CUT].astype(F32)
        else:
            acc = yb[0, 0, :, :, 2 * CUT : D].astype(F32)
        for o in (1, 2, 3):
            line = r1c[o - 1, 0] if part == 2 else r1[part][o - 1, :, 0]
            acc = acc + line.astype(F32)
        total[:, CUT * part : CUT * part + WIDTH[part]] += acc[0]
        for o in near:
            arrive("r2", part, o)
        acc = acc[1:4]
        for o in (1, 2, 3):
            acc = acc + r2[part][o - 1, 1:4].astype(F32)
        s2[part][1:4] = acc.astype(BF)
        for o in near:
            send(("r3", part, o), s2[part].at[o], r3[part].at[o - 1], part, o)
    drain("r1", "r1l", "r2", "r2l")
    for part in (2, 1, 0):
        for o in near:
            arrive("r2l", part, o)
        acc = r2[part][0, 0].astype(F32)
        for o in (2, 3):
            acc = acc + r2[part][o - 1, 0].astype(F32)
        for o in near:
            arrive("r3", part, o)
        for o in (1, 2, 3):
            acc = acc + r3[part][o - 1].astype(F32)
        total[:, CUT * part : CUT * part + WIDTH[part]] += acc

    summed = total[...]
    mean = jnp.mean(summed * summed, axis=-1, keepdims=True)
    mixed = jnp.where(live, summed * lax.rsqrt(mean + EPS) * og_ref[...], 0.0)
    mixed = mixed.astype(BF)
    for s in range(4):
        out_ref[s] = mixed[4 * s : 4 * s + 4, :]
    drain("r3")


def per_device(
    tokens, lengths, routes, gates, norm_gain,
    expert_gate, expert_up, expert_down, shared_gate, shared_up, shared_down, out_gain,
):
    vmem = pl.BlockSpec(memory_space=pltpu.VMEM)
    hbm = pl.BlockSpec(memory_space=pltpu.HBM)
    dma = pltpu.SemaphoreType.DMA
    buffers = [pltpu.VMEM((4, 4, 4, 16, WIDE), BF), pltpu.VMEM((4, 4, 4, 16, D), BF)]
    buffers += [pltpu.VMEM((3, 4, 4, 16, w), BF) for w in WIDTH]
    buffers += [pltpu.VMEM((4, 4, 16, w), BF) for w in WIDTH]
    buffers += [pltpu.VMEM((3, 4, 16, w), BF) for w in WIDTH]
    buffers += [pltpu.VMEM((4, 16, w), BF) for w in WIDTH]
    buffers += [pltpu.VMEM((3, 16, w), BF) for w in WIDTH]
    buffers += [
        pltpu.VMEM((4, D, 256), BF), pltpu.VMEM((4, D, 256), BF), pltpu.VMEM((4, 256, D), BF),
        pltpu.VMEM((D, 256), BF), pltpu.VMEM((D, 256), BF), pltpu.VMEM((256, D), BF),
        pltpu.VMEM((16, D), F32), pltpu.VMEM((16, 128), F32), pltpu.VMEM((16, 128), F32),
        pltpu.VMEM((256, D), BF), pltpu.VMEM((16, D), F32),
        pltpu.SMEM((4,), jnp.int32), pltpu.VMEM((4, 4, D), BF),
        pltpu.VMEM((4, 4, 8), jnp.int32), pltpu.VMEM((4, 4, 8), F32),
        pltpu.VMEM((1, D), F32), pltpu.VMEM((1, D), F32),
    ]
    return pl.pallas_call(
        kernel,
        out_shape=jax.ShapeDtypeStruct(tokens.shape, BF),
        in_specs=[hbm] * 12,
        out_specs=vmem,
        scratch_shapes=buffers
        + [dma((120,)), dma((120,)), dma((3,)), dma((3,)), dma((6,)), dma((6,))],
        compiler_params=pltpu.CompilerParams(
            collective_id=0, has_side_effects=True, vmem_limit_bytes=67043328
        ),
    )(
        lengths, tokens, routes, gates, norm_gain.reshape(1, D), out_gain.reshape(1, D),
        expert_gate, expert_up, expert_down, shared_gate, shared_up, shared_down,
    )


def solution(mesh):
    placed = (
        P("ep", None, None), P("ep"), P("ep", None, None), P("ep", None, None), P(),
        P("ep", None, None), P("ep", None, None), P("ep", None, None), P(), P(), P(), P(),
    )
    return jax.shard_map(
        per_device, mesh=mesh, in_specs=placed, out_specs=P("ep", None, None), check_vma=False
    )
```
